32 devices in a mesh: fs: 8 (over z, y), tp: 4 (over x, core).
Axes of the slice: x: 2, y: 2, z: 4, core: 2. Of those that a mesh axis runs over, the one named last changes fastest.
Arguments:
- inputs: bfloat16 [4096, 2304], P('fs'), may hold values from -6 to 6
- value_cot: bfloat16 [4096, 4096], P('fs', 'tp'), may hold values from -0.09375 to 0.09375
- retained: bfloat16 [4096, 4096], P('fs', 'tp'), may hold values from -6 to 6
- output_cot: bfloat16 [4096, 2304], P('fs'), may hold values from -0.09375 to 0.09375
- proj_value: bfloat16 [2304, 192], P('fs'), may hold values from -0.125 to 0.125
- proj_output: bfloat16 [2304, 192], P('fs'), may hold values from -0.125 to 0.125
- w_value: float32 [2304, 4096], P('fs', 'tp'), may hold values from -6 to 6
- w_output: float32 [4096, 2304], P('tp', 'fs'), may hold values from -6 to 6
- first_value: float32 [192, 4096], P('fs', 'tp'), may hold values from -106 to 106
- second_value: float32 [192, 4096], P('fs', 'tp'), may hold values from 0.25 to 4
- first_output: float32 [192, 4096], P('fs', 'tp'), may hold values from -106 to 106
- second_output: float32 [192, 4096], P('fs', 'tp'), may hold values from 0.25 to 4
Outputs:
- step_value: float32 [2304, 4096], P('fs', 'tp')
- step_output: float32 [4096, 2304], P('tp', 'fs')
- copy_value: bfloat16 [2304, 4096], P(None, 'tp')
- copy_output: bfloat16 [4096, 2304], P('tp')
- new_first_value: float32 [192, 4096], P('fs', 'tp')
- new_second_value: float32 [192, 4096], P('fs', 'tp')
- new_first_output: float32 [192, 4096], P('fs', 'tp')
- new_second_output: float32 [192, 4096], P('fs', 'tp')
The draws below stay inside these ranges and needn't reach their ends.
All inputs are finite; a program needn't handle non-finite values.
Results may differ from the reference program's by a relative error of at most 0.0034.
Values may be sent and summed in bfloat16 or wider, within the bound.
A program may use at most 64 MiB of HBM per device.

```python
import math
import jax
import jax.numpy as jnp
from jax import lax

D = 2304
RANK = 192
HV = 4096
TOKENS = 4096


def moment_law(key, row_total, col_total):
    row_pos = jnp.arange(row_total, dtype=jnp.float32) / row_total
    col_pos = jnp.arange(col_total, dtype=jnp.float32) / col_total
    drawn = jnp.clip(jax.random.normal(key, (row_total, col_total), jnp.float32), -6.0, 6.0)
    row_scale = 3.0 ** row_pos
    col_scale = 3.0 ** col_pos
    return drawn * row_scale[:, None] * col_scale[None, :]


def draw_first_value(key, part):
    return moment_law(jax.random.fold_in(key, 11), RANK, HV)


def draw_first_output(key, part):
    return moment_law(jax.random.fold_in(key, 23), RANK, HV)


def block_scale(own_key, dims, shards, least, largest):
    gain, own = 1.0, jax.random.fold_in(own_key, 6)
    for dim, parts in shards:
        steps = jnp.exp(jax.random.uniform(jax.random.fold_in(own, dim), (parts,), jnp.float32, least / len(shards), largest / len(shards)))
        gain = gain * jnp.repeat(steps, dims[dim] // parts).reshape([-1 if axis == dim else 1 for axis in range(len(dims))])
    return gain


def scatter_about(rng, shape, spread, most, shards=(), kind=jnp.bfloat16):
    values = jax.random.normal(rng, shape, jnp.float32) * spread
    if len(shards) > 0:
        values = block_scale(rng, shape, shards, -0.22, 0.18) * values
    return jnp.clip(values, min=-most, max=most).astype(kind)


def setup_inputs(seed: int = 0) -> dict:
    seeds = jax.random.split(jax.random.key(seed), 13)
    inputs = scatter_about(seeds[0], (TOKENS, D), 1.0, 6.0, ((0, 8),))
    value_cot = scatter_about(seeds[1], (TOKENS, HV), (TOKENS ** -0.5), 0.09375, ((0, 8), (1, 4)))
    retained = scatter_about(seeds[2], (TOKENS, HV), 1.0, 6.0, ((0, 8), (1, 4)))
    output_cot = scatter_about(seeds[3], (TOKENS, D), (TOKENS ** -0.5), 0.09375, ((0, 8),))
    proj_value = scatter_about(seeds[4], (D, RANK), D ** -0.5, 0.125, ((0, 8),))
    proj_output = scatter_about(seeds[5], (D, RANK), D ** -0.5, 0.125, ((0, 8),))
    w_value = scatter_about(seeds[6], (D, HV), 1.0, 6.0, ((0, 8), (1, 4)), jnp.float32)
    w_output = scatter_about(seeds[7], (HV, D), 1.0, 6.0, ((0, 4), (1, 8)), jnp.float32)
    first_value = draw_first_value(jax.random.fold_in(seeds[12], 71), 0)
    second_value = jnp.clip(jnp.exp(math.log(4.0) - 2.7725887 * jax.random.uniform(seeds[9], (RANK, HV), jnp.float32) ** block_scale(seeds[9], (RANK, HV), ((0, 8), (1, 4)), -0.2, 0.2)), 0.25, 4.0)
    first_output = draw_first_output(jax.random.fold_in(seeds[12], 71), 0)
    second_output = jnp.clip(jnp.exp(math.log(4.0) - 2.7725887 * jax.random.uniform(seeds[11], (RANK, HV), jnp.float32) ** block_scale(seeds[11], (RANK, HV), ((0, 8), (1, 4)), -0.2, 0.2)), 0.25, 4.0)
    return dict(inputs=inputs, value_cot=value_cot, retained=retained, output_cot=output_cot, proj_value=proj_value, proj_output=proj_output, w_value=w_value, w_output=w_output, first_value=first_value, second_value=second_value, first_output=first_output, second_output=second_output)


beta_one = 0.8
beta_two = 0.9
moment_eps = 1e-08
norm_eps = 1e-06

def adapt(first, second, grad):
    new_first = beta_one * first + (1.0 - beta_one) * grad
    new_second = beta_two * second + (1.0 - beta_two) * grad * grad
    direction = (new_first / (jnp.sqrt(new_second) + moment_eps)).astype(jnp.bfloat16)
    return (new_first, new_second, direction)

def reference(inputs, value_cot, retained, output_cot, proj_value, proj_output, w_value, w_output, first_value, second_value, first_output, second_output):
    x_proj = jnp.dot(inputs, proj_value, preferred_element_type=jnp.float32).astype(jnp.bfloat16)
    o_proj = jnp.dot(output_cot, proj_output, preferred_element_type=jnp.float32).astype(jnp.bfloat16)
    grad_value = jnp.dot(x_proj.T, value_cot, preferred_element_type=jnp.float32)
    grad_output = jnp.dot(o_proj.T, retained, preferred_element_type=jnp.float32)
    first_v, second_v, dir_value = adapt(first_value, second_value, grad_value)
    first_o, second_o, dir_output = adapt(first_output, second_output, grad_output)
    square_v = jnp.sum(jnp.square(dir_value.astype(jnp.float32)))
    square_o = jnp.sum(jnp.square(dir_output.astype(jnp.float32)))
    scale_value = lax.rsqrt(square_v / (RANK * HV) + norm_eps)
    scale_output = lax.rsqrt(square_o / (RANK * HV) + norm_eps)
    step_value = jnp.dot(proj_value, dir_value, preferred_element_type=jnp.float32) * scale_value
    step_output = jnp.dot(dir_output.T, proj_output.T, preferred_element_type=jnp.float32) * scale_output
    copy_value = (w_value + step_value).astype(jnp.bfloat16)
    copy_output = (w_output + step_output).astype(jnp.bfloat16)
    return (step_value, step_output, copy_value, copy_output, first_v, second_v, first_o, second_o)
```

```python
import functools

import jax
import jax.numpy as jnp
from jax import lax
from jax.experimental import pallas as pl
from jax.experimental.pallas import tpu as pltpu
from jax.sharding import PartitionSpec as P

BF16 = jnp.bfloat16
F32 = jnp.float32

beta_one = 0.8
beta_two = 0.9
moment_eps = 1e-08
norm_eps = 1e-06

PIECES = 12
EARLY = 2
DEPTH = 3
HOOKS = (3, 5, 6, 12, 17, 22, 27)


def adapt(first, second, grad):
    new_first = beta_one * first + (1.0 - beta_one) * grad
    new_second = beta_two * second + (1.0 - beta_two) * grad * grad
    direction = (new_first / (jnp.sqrt(new_second) + moment_eps)).astype(BF16)
    return (new_first, new_second, direction)


def flat(block):
    parts, rows, columns = block.shape
    if rows % 16 == 0:
        return block.reshape(parts * rows, columns)
    return block.astype(F32).reshape(parts * rows, columns).astype(block.dtype)


def cut(rows):
    if rows % (16 * PIECES) == 0:
        return PIECES, EARLY
    count = rows // 16
    return count, max(1, count * EARLY // PIECES)


def share(q, t):
    ways = t // 2
    return ways if q % (16 * ways) == 0 else 1


def schedule(levels, count, early):
    line, sent = [], {}
    for s in range(levels - 1):
        for i in range(count):
            sent[s + 1, i] = len(line)
            line.append((0, s, i))
        for i in range(count - early, count):
            line.append((1, s, i))
    over = {}
    slot = 0
    for i in list(range(count - early, count)) + list(range(count - early)):
        over[slot] = (0, i)
        slot += 1
    for j in range(1, levels):
        for i in range(count - early):
            slot = max(slot, sent[j, i] + 3)
            over[slot] = (j, i)
            slot += 1
    return line, over, max(len(line), slot)


def exchange(
    n, t, x_ref, oc_ref, vc_ref, ret_ref, pv_ref, po_ref, wv_ref, wo_ref, fv_ref, sv_ref, fo_ref, so_ref,
    wall, pall, dall, sq, nfv, nsv, nfo, nso,
    xin, pr, gsend, gacross, gpart, grecv,
    load_sem, p_send, p_recv, x_send, x_recv, core_send, core_recv, ga_send, ga_recv, g_send, g_recv,
    d_send, d_recv, q_send, q_recv, up_send, down_send, over_send, w_recv,
):
    me = lax.axis_index("fs")
    tp = lax.axis_index("tp")
    core = lax.rem(tp, 2)
    partner = tp + 1 - 2 * core
    x = tp // 2
    z, y = me // 2, lax.rem(me, 2)
    levels = n // 2
    across = me + 1 - 2 * y
    q, columns = wv_ref.shape
    rows = 2 * q
    rr = fv_ref.shape[0]
    count, early = cut(rows)
    size = rows // count
    ways = share(q, t)
    part_rows = q // ways

    def remote(src, dst, ssem, rsem, device):
        return pltpu.make_async_remote_copy(
            src_ref=src, dst_ref=dst, send_sem=ssem, recv_sem=rsem,
            device_id=device, device_id_type=pl.DeviceIdType.MESH,
        )

    barrier = pltpu.get_barrier_semaphore()
    for d in range(1, n):
        pl.semaphore_signal(
            barrier, inc=1, device_id={"fs": lax.rem(me + d, n)}, device_id_type=pl.DeviceIdType.MESH
        )
    for d in range(1, t):
        pl.semaphore_signal(
            barrier, inc=1, device_id={"tp": lax.rem(tp + d, t)}, device_id_type=pl.DeviceIdType.MESH
        )

    @pl.when(core == 0)
    def _():
        pltpu.make_async_copy(x_ref, xin, load_sem).start()
        pall[0, me] = pv_ref[...]

    @pl.when(core == 1)
    def _():
        pltpu.make_async_copy(oc_ref, xin, load_sem).start()
        pall[1, me] = po_ref[...]

    wall[me, :q] = wv_ref[...].astype(BF16)
    wall[me, q:] = wo_ref[...].astype(BF16)
    pl.semaphore_wait(barrier, n - 1 + t - 1)

    sends = []

    def go(copy):
        copy.start()
        sends.append(copy)
        return copy

    def spread(place, ssem, rsem):
        own = place(me)
        first = [go(remote(own, own, ssem.at[0], rsem.at[0], {"fs": across}))]
        for d in range(1, levels):
            target = lax.rem(z + d, levels) * 2 + y
            first.append(go(remote(own, own, ssem.at[d], rsem.at[d], {"fs": target})))
        return first

    def pass_on(first, place, ssem, rsem):
        second = []
        for d in range(1, levels):
            first[d].wait_recv()
            block = place(lax.rem(z + levels - d, levels) * 2 + y)
            second.append(
                go(remote(block, block, ssem.at[levels + d], rsem.at[levels + d], {"fs": across}))
            )
        return first[:1] + second

    line, over, slots = schedule(levels, count, early)

    def piece(level, side, i):
        column = y if side == 0 else 1 - y
        return wall.at[level * 2 + column, pl.ds(i * size, size)]

    def along(slot, step):
        side, s, i = line[slot]
        place = piece(z - s if step > 0 else z + s, side, i)
        ssem = (up_send if step > 0 else down_send).at[slot % DEPTH]
        level = z - s if step > 0 else z + s
        return remote(place, place, ssem, w_recv.at[side, level, i], {"fs": (z + step) * 2 + y})

    def goes(slot, step):
        s = line[slot][1]
        if step > 0:
            return jnp.logical_and(z >= s, z < levels - 1)
        return jnp.logical_and(z + s < levels, z > 0)

    def nearest(j):
        if j == 0:
            return z
        low = jnp.minimum(z, levels - 1 - z)
        near = z + (j + 1) // 2 * (1 if j % 2 else -1)
        far = jnp.where(z < levels - 1 - z, j, levels - 1 - j)
        return jnp.where(j <= 2 * low, near, far)

    def crossing(slot):
        j, i = over[slot]
        level = nearest(j)
        place = piece(level, 0, i)
        return remote(place, place, over_send.at[slot % DEPTH], w_recv.at[1, level, i], {"fs": across})

    held = set()

    def landed(side, level, i):
        place = piece(level, side, i)
        remote(place, place, over_send.at[0], w_recv.at[side, level, i], {"fs": across}).wait_recv()

    def ensure(side, k, i):
        if (side, k, i) in held:
            return
        held.add((side, k, i))
        if k == 0:
            landed(side, z, i)
            return

        @pl.when(z >= k)
        def _():
            landed(side, z - k, i)

        @pl.when(z + k < levels)
        def _():
            landed(side, z + k, i)

    def drained(slot):
        if 0 <= slot < len(line):
            for step in (1, -1):
                @pl.when(goes(slot, step))
                def _():
                    along(slot, step).wait_send()
        if slot in over:
            crossing(slot).wait_send()

    def advance(slot):
        drained(slot - DEPTH)
        if slot < len(line):
            side, s, i = line[slot]
            if side == 1 or s > 0:
                ensure(side, s, i)
            for step in (1, -1):
                @pl.when(goes(slot, step))
                def _():
                    along(slot, step).start()
        if slot in over:
            j, i = over[slot]
            for k in range(1, j + 1):
                ensure(0, k, i)
            crossing(slot).start()

    chain = {}

    def part(block):
        return pall.at[core, block, pl.ds(x * part_rows, part_rows)]

    def shared(block):
        for d in range(1, ways):
            place = part(block)
            target = lax.rem(x + d, ways) * 2 + core
            chain["shared"].append(
                go(remote(place, place, x_send.at[d, block], x_recv.at[d, block], {"tp": target}))
            )

    def hook_pass():
        first = chain["proj"]
        second = pass_on(first, part, p_send, p_recv)
        for d in range(1, levels):
            shared(lax.rem(z + levels - d, levels) * 2 + y)
        chain["proj"] = second

    def hook_share():
        second = chain["proj"]
        for d, copy in enumerate(second):
            copy.wait_recv()
            shared(lax.rem(z + levels - d, levels) * 2 + 1 - y)

    def hook_grads():
        for copy in chain["shared"]:
            copy.wait_recv()
        chain["whole"] = go(
            remote(pall.at[core], pall.at[core], core_send.at[0], core_recv.at[0], {"tp": partner})
        )
        pltpu.make_async_copy(x_ref, xin, load_sem).wait()
        pr[core] = jnp.dot(xin[...], flat(pall[core]), preferred_element_type=F32).astype(BF16)
        swapped = go(remote(pr.at[core], pr.at[core], core_send.at[1], core_recv.at[1], {"tp": partner}))
        swapped.wait_recv()
        for side, cot in ((0, vc_ref), (1, ret_ref)):
            grad = lax.dot_general(
                pr[side], cot[...], (((0,), (0,)), ((), ())), preferred_element_type=F32
            )
            for peer in range(n):
                gsend[peer % 2, peer // 2, :, side * columns:(side + 1) * columns] = (
                    grad[peer * rr:(peer + 1) * rr].astype(BF16)
                )
        chain["ga"] = go(
            remote(gsend.at[1 - y], gacross, ga_send.at[0], ga_recv.at[0], {"fs": across})
        )

    def hook_partial():
        chain["ga"].wait_recv()
        gpart[...] = (gsend[y].astype(F32) + gacross[...].astype(F32)).astype(BF16)
        copies = []
        for d in range(1, levels):
            level = lax.rem(z + d, levels)
            copies.append(
                go(remote(gpart.at[level], grecv.at[z], g_send.at[d], g_recv.at[d], {"fs": level * 2 + y}))
            )
        chain["g"] = copies

    def hook_moments():
        for copy in chain["g"]:
            copy.wait_recv()
        total = gsend[y, z].astype(F32) + gacross[z].astype(F32)
        for d in range(1, levels):
            total += grecv[lax.rem(z + levels - d, levels)].astype(F32)
        for side, refs in ((0, (fv_ref, sv_ref, nfv, nsv)), (1, (fo_ref, so_ref, nfo, nso))):
            grad = total[:, side * columns:(side + 1) * columns]
            new_first, new_second, direction = adapt(refs[0][...], refs[1][...], grad)
            refs[2][...] = new_first
            refs[3][...] = new_second
            dall[me, :, side * columns:(side + 1) * columns] = direction
        chain["dirs"] = spread(lambda block: dall.at[block], d_send, d_recv)

    def hook_dirs():
        chain["dirs"] = pass_on(chain["dirs"], lambda block: dall.at[block], d_send, d_recv)

    def hook_sums():
        for copy in chain["dirs"]:
            copy.wait_recv()
        sums = []
        for side in (0, 1):
            acc = jnp.zeros((rr, columns), F32)
            for k in range(n):
                acc += jnp.square(dall[k, :, side * columns:(side + 1) * columns].astype(F32))
            sums.append(jnp.sum(acc))
        row = lax.broadcasted_iota(jnp.int32, sq.shape[1:], 0)
        sq[tp] = jnp.where(row == 0, sums[0], sums[1])
        chain["sq"] = [
            go(remote(sq.at[tp], sq.at[tp], q_send.at[d], q_recv.at[d], {"tp": lax.rem(tp + d, t)}))
            for d in range(1, t)
        ]

    hooks = dict(zip(
        HOOKS, (hook_pass, hook_share, hook_grads, hook_partial, hook_moments, hook_dirs, hook_sums)
    ))
    chain["shared"] = []
    chain["proj"] = spread(part, p_send, p_recv)
    end = max(slots, max(HOOKS) + 1)
    for slot in range(end):
        if slot in hooks:
            hooks[slot]()
        advance(slot)
    for slot in range(end, slots + DEPTH):
        drained(slot - DEPTH)

    for k in range(1, levels):
        for i in range(count):
            ensure(0, k, i)
        for i in range(count - early, count):
            ensure(1, k, i)
    for j in range(levels):
        for i in range(count - early):
            landed(1, nearest(j), i)
    for copy in chain["sq"]:
        copy.wait_recv()
    chain["whole"].wait_recv()
    for copy in sends:
        copy.wait_send()


def finish(q, count, sq_ref, wall_ref, pall_ref, own_v, own_o, dv_ref, do_ref, step_v, step_o, copy_v, copy_o):
    totals = jnp.sum(sq_ref[...], axis=0)
    scale_v = lax.rsqrt(totals[0:1, 0:1] / count + norm_eps)
    scale_o = lax.rsqrt(totals[1:2, 0:1] / count + norm_eps)
    n, _, lanes = wall_ref.shape
    dir_v, dir_o = dv_ref[...], do_ref[...]
    step_v[...] = jnp.dot(own_v[...], dir_v, preferred_element_type=F32) * scale_v
    step_o[...] = jnp.dot(own_o[...], dir_o, preferred_element_type=F32) * scale_o
    w_v = wall_ref[:, :q].astype(F32).reshape(n * q, lanes)
    w_o = wall_ref[:, q:].astype(F32).reshape(n * q, lanes)
    copy_v[...] = (
        w_v + jnp.dot(pall_ref[0], dir_v, preferred_element_type=F32) * scale_v
    ).astype(BF16)
    moved = w_o + jnp.dot(pall_ref[1], dir_o, preferred_element_type=F32) * scale_o
    copy_o[...] = moved.T.astype(BF16)


def per_device(
    n, t,
    inputs, value_cot, retained, output_cot, proj_value, proj_output, w_value, w_output,
    first_value, second_value, first_output, second_output,
):
    tokens, width = inputs.shape
    q, rank = proj_value.shape
    columns = value_cot.shape[1]
    rr = first_value.shape[0]
    levels = n // 2
    pieces, _ = cut(2 * q)
    ways = share(q, t)
    vmem = pl.BlockSpec(memory_space=pltpu.VMEM)
    anywhere = pl.BlockSpec(memory_space=pl.ANY)
    dma = pltpu.SemaphoreType.DMA
    moment = jax.ShapeDtypeStruct((rr, columns), F32)
    wall, pall, dall, sq, first_v, second_v, first_o, second_o = pl.pallas_call(
        functools.partial(exchange, n, t),
        out_shape=(
            jax.ShapeDtypeStruct((n, 2 * q, columns), BF16),
            jax.ShapeDtypeStruct((2, n, q, rank), BF16),
            jax.ShapeDtypeStruct((n, rr, 2 * columns), BF16),
            jax.ShapeDtypeStruct((t, 8, 128), F32),
            moment, moment, moment, moment,
        ),
        in_specs=[anywhere, anywhere] + [vmem] * 10,
        out_specs=(vmem,) * 8,
        scratch_shapes=[
            pltpu.VMEM((tokens, width), BF16),
            pltpu.VMEM((2, tokens, rank), BF16),
            pltpu.VMEM((2, levels, rr, 2 * columns), BF16),
            pltpu.VMEM((levels, rr, 2 * columns), BF16),
            pltpu.VMEM((levels, rr, 2 * columns), BF16),
            pltpu.VMEM((levels, rr, 2 * columns), BF16),
            dma, dma((n,)), dma((n,)), dma((ways, n)), dma((ways, n)), dma((2,)), dma((2,)),
            dma((1,)), dma((1,)), dma((levels,)), dma((levels,)), dma((n,)), dma((n,)),
            dma((t,)), dma((t,)),
            dma((DEPTH,)), dma((DEPTH,)), dma((DEPTH,)), dma((2, levels, pieces)),
        ],
        compiler_params=pltpu.CompilerParams(
            collective_id=0, has_side_effects=True, vmem_limit_bytes=60 * 1024 * 1024
        ),
        name="exchange",
    )(
        inputs, output_cot, value_cot, retained, proj_value, proj_output, w_value, w_output.T,
        first_value, second_value, first_output, second_output,
    )
    lanes = 128
    tiles = columns // lanes
    dirs = dall.reshape(n * rr, 2 * columns)
    full = n * q
    step_v, step_o, copy_v, copy_o = pl.pallas_call(
        functools.partial(finish, q, float(rank * columns * t)),
        grid=(tiles,),
        out_shape=(
            jax.ShapeDtypeStruct((q, columns), F32),
            jax.ShapeDtypeStruct((q, columns), F32),
            jax.ShapeDtypeStruct((full, columns), BF16),
            jax.ShapeDtypeStruct((columns, full), BF16),
        ),
        in_specs=[
            pl.BlockSpec((t, 8, 128), lambda j: (0, 0, 0)),
            pl.BlockSpec((n, 2 * q, lanes), lambda j: (0, 0, j)),
            pl.BlockSpec((2, full, rank), lambda j: (0, 0, 0)),
            pl.BlockSpec((q, rank), lambda j: (0, 0)),
            pl.BlockSpec((q, rank), lambda j: (0, 0)),
            pl.BlockSpec((rank, lanes), lambda j: (0, j)),
            pl.BlockSpec((rank, lanes), lambda j: (0, j + tiles)),
        ],
        out_specs=(
            pl.BlockSpec((q, lanes), lambda j: (0, j)),
            pl.BlockSpec((q, lanes), lambda j: (0, j)),
            pl.BlockSpec((full, lanes), lambda j: (0, j)),
            pl.BlockSpec((lanes, full), lambda j: (j, 0)),
        ),
        compiler_params=pltpu.CompilerParams(vmem_limit_bytes=48 * 1024 * 1024),
        name="finish",
    )(sq, wall, pall.reshape(2, full, rank), proj_value, proj_output, dirs, dirs)
    return (step_v, step_o.T, copy_v, copy_o, first_v, second_v, first_o, second_o)


def solution(mesh):
    in_specs = (
        P("fs", None),
        P("fs", "tp"),
        P("fs", "tp"),
        P("fs", None),
        P("fs", None),
        P("fs", None),
        P("fs", "tp"),
        P("tp", "fs"),
        P("fs", "tp"),
        P("fs", "tp"),
        P("fs", "tp"),
        P("fs", "tp"),
    )
    out_specs = (
        P("fs", "tp"),
        P("tp", "fs"),
        P(None, "tp"),
        P("tp", None),
        P("fs", "tp"),
        P("fs", "tp"),
        P("fs", "tp"),
        P("fs", "tp"),
    )
    return jax.shard_map(
        functools.partial(per_device, mesh.shape["fs"], mesh.shape["tp"]),
        mesh=mesh, in_specs=in_specs, out_specs=out_specs, check_vma=False,
    )
```

```python
import functools

import jax
import jax.numpy as jnp
from jax import lax
from jax.experimental import pallas as pl
from jax.experimental.pallas import tpu as pltpu
from jax.sharding import PartitionSpec as P

BF16 = jnp.bfloat16
F32 = jnp.float32

beta_one = 0.8
beta_two = 0.9
moment_eps = 1e-08
norm_eps = 1e-06

PIECES = 12
EARLY = 2
DEPTH = 5
HOOKS = (3, 5, 8, 16, 23, 30, 34, 37)
LAG = 3
UNITS = 2
STREAMED = 8


def adapt(first, second, grad):
    new_first = beta_one * first + (1.0 - beta_one) * grad
    new_second = beta_two * second + (1.0 - beta_two) * grad * grad
    direction = (new_first / (jnp.sqrt(new_second) + moment_eps)).astype(BF16)
    return (new_first, new_second, direction)


def flat(block):
    parts, rows, columns = block.shape
    if rows % 16 == 0:
        return block.reshape(parts * rows, columns)
    return block.astype(F32).reshape(parts * rows, columns).astype(block.dtype)


def cut(rows):
    if rows % (16 * PIECES) == 0:
        return PIECES, EARLY
    count = rows // 16
    return count, max(1, count * EARLY // PIECES)


def share(q, t):
    ways = t // 2
    return ways if q % (16 * ways) == 0 else 1


def schedule(levels, count, early):
    line, sent = [], {}
    for s in range(levels - 1):
        for i in range(count):
            sent[s + 1, i] = len(line)
            line.append((0, s, i))
        for i in range(count - early, count):
            line.append((1, s, i))
    over = {}
    slot = 0
    for i in list(range(count - early, count)) + list(range(count - early)):
        over[slot] = (0, i)
        slot += 1
    for j in range(1, levels):
        for i in range(count - early):
            slot = max(slot, sent[j, i] + 3)
            over[slot] = (j, i)
            slot += 1
    return line, over, max(len(line), slot)


def exchange(
    n, t, x_ref, oc_ref, vc_ref, ret_ref, pv_ref, po_ref, wv_ref, wo_ref, fv_ref, sv_ref, fo_ref, so_ref,
    copy_v, copy_o, step_v, step_o, nfv, nsv, nfo, nso,
    wall, own, pall, xin, cot, old, pr, gsend, gacross, gpart, grecv, dall, dir32, dirs, sq, scales,
    load_sem, p_send, p_recv, x_send, x_recv, core_send, core_recv, ga_send, ga_recv, g_send, g_recv,
    d_send, d_recv, q_send, q_recv, up_send, down_send, over_send, w_recv,
):
    me = lax.axis_index("fs")
    tp = lax.axis_index("tp")
    core = lax.rem(tp, 2)
    partner = tp + 1 - 2 * core
    x = tp // 2
    z, y = me // 2, lax.rem(me, 2)
    levels = n // 2
    across = me + 1 - 2 * y
    q, columns = wv_ref.shape
    rows = 2 * q
    rr, rank = fv_ref.shape[0], pv_ref.shape[1]
    count, early = cut(rows)
    size = rows // count
    ways = share(q, t)
    part_rows = q // ways
    streamed = levels <= STREAMED

    def remote(src, dst, ssem, rsem, device):
        return pltpu.make_async_remote_copy(
            src_ref=src, dst_ref=dst, send_sem=ssem, recv_sem=rsem,
            device_id=device, device_id_type=pl.DeviceIdType.MESH,
        )

    barrier = pltpu.get_barrier_semaphore()
    for d in range(1, n):
        pl.semaphore_signal(
            barrier, inc=1, device_id={"fs": lax.rem(me + d, n)}, device_id_type=pl.DeviceIdType.MESH
        )
    for d in range(1, t):
        pl.semaphore_signal(
            barrier, inc=1, device_id={"tp": lax.rem(tp + d, t)}, device_id_type=pl.DeviceIdType.MESH
        )

    @pl.when(core == 0)
    def _():
        pltpu.make_async_copy(pv_ref, pall.at[0, me], load_sem.at[0]).start()

    @pl.when(core == 1)
    def _():
        pltpu.make_async_copy(po_ref, pall.at[1, me], load_sem.at[0]).start()

    def load(src, dst, k):
        copy = pltpu.make_async_copy(src, dst, load_sem.at[k])
        copy.start()
        return copy

    weights = [load(wv_ref, own.at[0], 1), load(wo_ref, own.at[1], 2)]

    @pl.when(core == 0)
    def _():
        pltpu.make_async_copy(x_ref, xin, load_sem.at[3]).start()

    @pl.when(core == 1)
    def _():
        pltpu.make_async_copy(oc_ref, xin, load_sem.at[3]).start()

    cots = [load(vc_ref, cot.at[0], 4), load(ret_ref, cot.at[1], 5)]
    olds = [load(ref, old.at[k], 6 + k) for k, ref in enumerate((fv_ref, sv_ref, fo_ref, so_ref))]

    pltpu.make_async_copy(pv_ref, pall.at[core, me], load_sem.at[0]).wait()
    pl.semaphore_wait(barrier, n - 1 + t - 1)

    sends = []

    def go(copy):
        copy.start()
        sends.append(copy)
        return copy

    def spread(place, ssem, rsem):
        mine = place(me)
        first = [go(remote(mine, mine, ssem.at[0], rsem.at[0], {"fs": across}))]
        for d in range(1, levels):
            target = lax.rem(z + d, levels) * 2 + y
            first.append(go(remote(mine, mine, ssem.at[d], rsem.at[d], {"fs": target})))
        return first

    def pass_on(first, place, ssem, rsem):
        second = []
        for d in range(1, levels):
            first[d].wait_recv()
            block = place(lax.rem(z + levels - d, levels) * 2 + y)
            second.append(
                go(remote(block, block, ssem.at[levels + d], rsem.at[levels + d], {"fs": across}))
            )
        return first[:1] + second

    line, over, slots = schedule(levels, count, early)

    def piece(level, side, i):
        column = y if side == 0 else 1 - y
        return wall.at[level * 2 + column, pl.ds(i * size, size)]

    def along(slot, step):
        side, s, i = line[slot]
        level = z - s if step > 0 else z + s
        place = piece(level, side, i)
        ssem = (up_send if step > 0 else down_send).at[slot % DEPTH]
        return remote(place, place, ssem, w_recv.at[side, level, i], {"fs": (z + step) * 2 + y})

    def goes(slot, step):
        s = line[slot][1]
        if step > 0:
            return jnp.logical_and(z >= s, z < levels - 1)
        return jnp.logical_and(z + s < levels, z > 0)

    def nearest(j):
        if j == 0:
            return z
        low = jnp.minimum(z, levels - 1 - z)
        near = z + (j + 1) // 2 * (1 if j % 2 else -1)
        far = jnp.where(z < levels - 1 - z, j, levels - 1 - j)
        return jnp.where(j <= 2 * low, near, far)

    def crossing(slot):
        j, i = over[slot]
        level = nearest(j)
        place = piece(level, 0, i)
        return remote(place, place, over_send.at[slot % DEPTH], w_recv.at[1, level, i], {"fs": across})

    held = set()

    def landed(side, level, i):
        place = piece(level, side, i)
        remote(place, place, over_send.at[0], w_recv.at[side, level, i], {"fs": across}).wait_recv()

    def ensure(side, k, i):
        if (side, k, i) in held:
            return
        held.add((side, k, i))
        if k == 0:
            landed(side, z, i)
            return

        @pl.when(z >= k)
        def _():
            landed(side, z - k, i)

        @pl.when(z + k < levels)
        def _():
            landed(side, z + k, i)

    def crossed(j, i):
        if ("over", j, i) not in held:
            held.add(("over", j, i))
            landed(1, nearest(j), i)

    def drained(slot):
        if 0 <= slot < len(line):
            for step in (1, -1):
                @pl.when(goes(slot, step))
                def _():
                    along(slot, step).wait_send()
        if slot in over:
            crossing(slot).wait_send()

    def advance(slot):
        drained(slot - DEPTH)
        if slot < len(line):
            side, s, i = line[slot]
            if side == 1 or s > 0:
                ensure(side, s, i)
            for step in (1, -1):
                @pl.when(goes(slot, step))
                def _():
                    along(slot, step).start()
        if slot in over:
            j, i = over[slot]
            for k in range(1, j + 1):
                ensure(0, k, i)
            crossing(slot).start()

    copies, steps = (copy_v, copy_o), (step_v, step_o)

    def moved(block, side, low, high):
        part = jnp.dot(pall[side, block, low:high], dirs[side], preferred_element_type=F32)
        return part * scales[side, 0:1, 0:1]

    def renew(block, side, low, high):
        old_part = wall[block, side * q + low:side * q + high].astype(F32)
        copies[side][block, low:high] = (old_part + moved(block, side, low, high)).astype(BF16)

    def renew_own(side):
        step = moved(me, side, 0, q)
        steps[side][...] = step
        copies[side][me] = (own[side] + step).astype(BF16)

    def unit(side, j, half, low, high):
        if side == 0 and j == 0:
            renew_own(half)
            return
        for i in range((half * q + low) // size, -(-(half * q + high) // size)):
            if side == 1 and (i < count - early or j == 0):
                if i < count - early:
                    crossed(j, i)
                else:
                    ensure(1, 0, i)
            else:
                for k in range(1, j + 1):
                    ensure(side, k, i)
        renew(nearest(j) * 2 + (y if side == 0 else 1 - y), half, low, high)

    def plan():
        at_line = {item: slot for slot, item in enumerate(line)}
        at_over = {item: slot for slot, item in over.items()}
        units = []
        for j in range(levels):
            for side in (0, 1):
                fine = 2 * size if j == levels - 1 and q % (2 * size) == 0 else q
                for half in (0, 1):
                    for low in range(0, q, fine):
                        ready = 0
                        for i in range((half * q + low) // size, -(-(half * q + low + fine) // size)):
                            if side == 1 and (j == 0 or i < count - early):
                                ready = max(ready, at_over[j, i] + LAG)
                            elif j > 0:
                                ready = max(ready, at_line[side, j - 1, i] + LAG)
                        units.append((ready, len(units), (side, j, half, low, low + fine)))
        return sorted(units)

    chain = {}

    def part(block):
        return pall.at[core, block, pl.ds(x * part_rows, part_rows)]

    def shared(block):
        for d in range(1, ways):
            place = part(block)
            target = lax.rem(x + d, ways) * 2 + core
            chain["shared"].append(
                go(remote(place, place, x_send.at[d, block], x_recv.at[d, block], {"tp": target}))
            )

    def hook_pass():
        first = chain["proj"]
        second = pass_on(first, part, p_send, p_recv)
        for d in range(1, levels):
            shared(lax.rem(z + levels - d, levels) * 2 + y)
        chain["proj"] = second

    def hook_share():
        second = chain["proj"]
        for d, copy in enumerate(second):
            copy.wait_recv()
            shared(lax.rem(z + levels - d, levels) * 2 + 1 - y)

    def hook_grads():
        for copy in chain["shared"]:
            copy.wait_recv()
        chain["whole"] = go(
            remote(pall.at[core], pall.at[core], core_send.at[0], core_recv.at[0], {"tp": partner})
        )
        pltpu.make_async_copy(x_ref, xin, load_sem.at[3]).wait()
        pr[core] = jnp.dot(xin[...], flat(pall[core]), preferred_element_type=F32).astype(BF16)
        swapped = go(remote(pr.at[core], pr.at[core], core_send.at[1], core_recv.at[1], {"tp": partner}))
        for copy in cots:
            copy.wait()
        swapped.wait_recv()
        for side in (0, 1):
            grad = lax.dot_general(
                pr[side], cot[side], (((0,), (0,)), ((), ())), preferred_element_type=F32
            )
            for peer in range(n):
                gsend[peer % 2, peer // 2, :, side * columns:(side + 1) * columns] = (
                    grad[peer * rr:(peer + 1) * rr].astype(BF16)
                )
        chain["ga"] = go(
            remote(gsend.at[1 - y], gacross, ga_send.at[0], ga_recv.at[0], {"fs": across})
        )

    def hook_partial():
        chain["ga"].wait_recv()
        gpart[...] = (gsend[y].astype(F32) + gacross[...].astype(F32)).astype(BF16)
        copies = []
        for d in range(1, levels):
            level = lax.rem(z + d, levels)
            copies.append(
                go(remote(gpart.at[level], grecv.at[z], g_send.at[d], g_recv.at[d], {"fs": level * 2 + y}))
            )
        chain["g"] = copies

    def hook_moments():
        for copy in olds:
            copy.wait()
        for copy in chain["g"]:
            copy.wait_recv()
        total = gsend[y, z].astype(F32) + gacross[z].astype(F32)
        for d in range(1, levels):
            total += grecv[lax.rem(z + levels - d, levels)].astype(F32)
        for side, refs in ((0, (nfv, nsv)), (1, (nfo, nso))):
            grad = total[:, side * columns:(side + 1) * columns]
            new_first, new_second, direction = adapt(old[2 * side], old[2 * side + 1], grad)
            refs[0][...] = new_first
            refs[1][...] = new_second
            dall[me, :, side * columns:(side + 1) * columns] = direction
        chain["dirs"] = spread(lambda block: dall.at[block], d_send, d_recv)

    def hook_dirs():
        chain["dirs"] = pass_on(chain["dirs"], lambda block: dall.at[block], d_send, d_recv)

    def hook_sums():
        for copy in chain["dirs"]:
            copy.wait_recv()
        sums = []
        for side in (0, 1):
            for k in range(n):
                dir32[k * rr:(k + 1) * rr] = dall[k, :, side * columns:(side + 1) * columns].astype(F32)
            whole = dir32[...]
            sums.append(jnp.sum(jnp.square(whole)))
            dirs[side] = whole.astype(BF16)
        row = lax.broadcasted_iota(jnp.int32, sq.shape[1:], 0)
        sq[tp] = jnp.where(row == 0, sums[0], sums[1])
        chain["sq"] = [
            go(remote(sq.at[tp], sq.at[tp], q_send.at[d], q_recv.at[d], {"tp": lax.rem(tp + d, t)}))
            for d in range(1, t)
        ]

    def hook_scales():
        for copy in chain["sq"]:
            copy.wait_recv()
        chain["whole"].wait_recv()
        totals = jnp.sum(sq[...], axis=0)
        spread_scales = lax.rsqrt(totals / float(rank * columns * t) + norm_eps)
        for side in (0, 1):
            scales[side] = jnp.broadcast_to(spread_scales[side:side + 1], scales.shape[1:])

    hooks = dict(zip(HOOKS, (
        hook_pass, hook_share, hook_grads, hook_partial, hook_moments, hook_dirs, hook_sums, hook_scales
    )))
    chain["shared"] = []
    chain["proj"] = spread(part, p_send, p_recv)
    for side in (0, 1):
        weights[side].wait()
        wall[me, side * q:(side + 1) * q] = own[side].astype(BF16)
    units = plan() if streamed else []
    end = max(slots, max(HOOKS) + 1)
    for slot in range(end):
        if slot in hooks:
            hooks[slot]()
        advance(slot)
        if slot >= max(HOOKS):
            for _ in range(UNITS):
                if units and units[0][0] <= slot:
                    unit(*units.pop(0)[2])
    for _, _, args in units:
        unit(*args)
    for slot in range(end, slots + DEPTH):
        drained(slot - DEPTH)

    for k in range(1, levels):
        for i in range(count):
            ensure(0, k, i)
        for i in range(count - early, count):
            ensure(1, k, i)
    for i in range(count - early, count):
        ensure(1, 0, i)
    for j in range(levels):
        for i in range(count - early):
            crossed(j, i)
    if not streamed:
        def whole_block(block, carry):
            for side in (0, 1):
                renew(block, side, 0, q)
            return carry

        lax.fori_loop(0, n, whole_block, 0)
        for side in (0, 1):
            renew_own(side)
    for copy in sends:
        copy.wait_send()


def finish(
    o_ref, v_ref, step_v, step_o, nfv, nsv, nfo, nso,
    copy_o, copy_v, out_v, out_o, first_v, second_v, first_o, second_o, sem,
):
    pairs = (
        (v_ref, copy_v), (step_v, out_v), (step_o, out_o),
        (nfv, first_v), (nsv, second_v), (nfo, first_o), (nso, second_o),
    )
    copies = [pltpu.make_async_copy(src, dst, sem.at[k]) for k, (src, dst) in enumerate(pairs)]

    @pl.when(pl.program_id(0) == 0)
    def _():
        for copy in copies:
            copy.start()

    parts, q, lanes = o_ref.shape
    copy_o[...] = o_ref[...].astype(F32).reshape(parts * q, lanes).T.astype(BF16)

    @pl.when(pl.program_id(0) == pl.num_programs(0) - 1)
    def _():
        for copy in copies:
            copy.wait()


def per_device(
    n, t,
    inputs, value_cot, retained, output_cot, proj_value, proj_output, w_value, w_output,
    first_value, second_value, first_output, second_output,
):
    tokens, width = inputs.shape
    q, rank = proj_value.shape
    columns = value_cot.shape[1]
    rr = first_value.shape[0]
    levels = n // 2
    pieces, _ = cut(2 * q)
    ways = share(q, t)
    hbm = pl.BlockSpec(memory_space=pltpu.HBM)
    vmem = pl.BlockSpec(memory_space=pltpu.VMEM)
    anywhere = pl.BlockSpec(memory_space=pl.ANY)
    dma = pltpu.SemaphoreType.DMA
    results = pl.pallas_call(
        functools.partial(exchange, n, t),
        out_shape=(
            pltpu.VMEM((n, q, columns), BF16),
            pltpu.VMEM((n, q, columns), BF16),
            pltpu.VMEM((q, columns), F32),
            pltpu.VMEM((q, columns), F32),
            pltpu.VMEM((rr, columns), F32),
            pltpu.VMEM((rr, columns), F32),
            pltpu.VMEM((rr, columns), F32),
            pltpu.VMEM((rr, columns), F32),
        ),
        in_specs=[hbm] * 12,
        out_specs=(vmem,) * 8,
        scratch_shapes=[
            pltpu.VMEM((n, 2 * q, columns), BF16),
            pltpu.VMEM((2, q, columns), F32),
            pltpu.VMEM((2, n, q, rank), BF16),
            pltpu.VMEM((tokens, width), BF16),
            pltpu.VMEM((2, tokens, columns), BF16),
            pltpu.VMEM((4, rr, columns), F32),
            pltpu.VMEM((2, tokens, rank), BF16),
            pltpu.VMEM((2, levels, rr, 2 * columns), BF16),
            pltpu.VMEM((levels, rr, 2 * columns), BF16),
            pltpu.VMEM((levels, rr, 2 * columns), BF16),
            pltpu.VMEM((levels, rr, 2 * columns), BF16),
            pltpu.VMEM((n, rr, 2 * columns), BF16),
            pltpu.VMEM((rank, columns), F32),
            pltpu.VMEM((2, rank, columns), BF16),
            pltpu.VMEM((t, 8, 128), F32),
            pltpu.VMEM((2, 8, 128), F32),
            dma((10,)), dma((n,)), dma((n,)), dma((ways, n)), dma((ways, n)), dma((2,)), dma((2,)),
            dma((1,)), dma((1,)), dma((levels,)), dma((levels,)), dma((n,)), dma((n,)),
            dma((t,)), dma((t,)),
            dma((DEPTH,)), dma((DEPTH,)), dma((DEPTH,)), dma((2, levels, pieces)),
        ],
        compiler_params=pltpu.CompilerParams(
            collective_id=0, has_side_effects=True, vmem_limit_bytes=51 * 1024 * 1024
        ),
        name="exchange",
    )(
        inputs, output_cot, value_cot, retained, proj_value, proj_output, w_value, w_output.T,
        first_value, second_value, first_output, second_output,
    )
    copy_v, copy_o, step_v, step_o = results[:4]
    lanes = 128
    full = n * q
    step = jax.ShapeDtypeStruct((q, columns), F32)
    moment = jax.ShapeDtypeStruct((rr, columns), F32)
    copy_o, copy_v, step_v, step_o, first_v, second_v, first_o, second_o = pl.pallas_call(
        finish,
        grid=(columns // lanes,),
        out_shape=(
            jax.ShapeDtypeStruct((columns, full), BF16),
            jax.ShapeDtypeStruct((full, columns), BF16),
            step, step, moment, moment, moment, moment,
        ),
        in_specs=[pl.BlockSpec((n, q, lanes), lambda j: (0, 0, j))] + [anywhere] * 7,
        out_specs=(pl.BlockSpec((lanes, full), lambda j: (j, 0)),) + (anywhere,) * 7,
        scratch_shapes=[dma((7,))],
        compiler_params=pltpu.CompilerParams(vmem_limit_bytes=12 * 1024 * 1024),
        name="finish",
    )(copy_o, copy_v.reshape(full, columns), step_v, step_o, *results[4:])
    return (step_v, step_o.T, copy_v, copy_o, first_v, second_v, first_o, second_o)


def solution(mesh):
    in_specs = (
        P("fs", None),
        P("fs", "tp"),
        P("fs", "tp"),
        P("fs", None),
        P("fs", None),
        P("fs", None),
        P("fs", "tp"),
        P("tp", "fs"),
        P("fs", "tp"),
        P("fs", "tp"),
        P("fs", "tp"),
        P("fs", "tp"),
    )
    out_specs = (
        P("fs", "tp"),
        P("tp", "fs"),
        P(None, "tp"),
        P("tp", None),
        P("fs", "tp"),
        P("fs", "tp"),
        P("fs", "tp"),
        P("fs", "tp"),
    )
    return jax.shard_map(
        functools.partial(per_device, mesh.shape["fs"], mesh.shape["tp"]),
        mesh=mesh, in_specs=in_specs, out_specs=out_specs, check_vma=False,
    )
```

```python
import functools

import jax
import jax.numpy as jnp
from jax import lax
from jax.experimental import pallas as pl
from jax.experimental.pallas import tpu as pltpu
from jax.sharding import PartitionSpec as P

BF16 = jnp.bfloat16
F32 = jnp.float32

beta_one = 0.8
beta_two = 0.9
moment_eps = 1e-08
norm_eps = 1e-06

PIECES = 12
EARLY = 2
DEPTH = 5
HOOKS = (3, 5, 8, 16, 23, 30, 34, 37)
LAG = 3
UNITS = 4
LANES = 128
DEEP = 12
SPLIT = 2
STREAMED = 8


def adapt(first, second, grad):
    new_first = beta_one * first + (1.0 - beta_one) * grad
    new_second = beta_two * second + (1.0 - beta_two) * grad * grad
    direction = (new_first / (jnp.sqrt(new_second) + moment_eps)).astype(BF16)
    return (new_first, new_second, direction)


def flat(block):
    parts, rows, columns = block.shape
    if rows % 16 == 0:
        return block.reshape(parts * rows, columns)
    return block.astype(F32).reshape(parts * rows, columns).astype(block.dtype)


def cut(rows):
    if rows % (16 * PIECES) == 0:
        return PIECES, EARLY
    count = rows // 16
    return count, max(1, count * EARLY // PIECES)


def share(q, t):
    ways = t // 2
    return ways if q % (16 * ways) == 0 else 1


def schedule(levels, count, early):
    line, sent = [], {}
    for s in range(levels - 1):
        for i in range(count):
            sent[s + 1, i] = len(line)
            line.append((0, s, i))
        for i in range(count - early, count):
            line.append((1, s, i))
    over = {}
    slot = 0
    for i in list(range(count - early, count)) + list(range(count - early)):
        over[slot] = (0, i)
        slot += 1
    for j in range(1, levels):
        for i in range(count - early):
            slot = max(slot, sent[j, i] + 3)
            over[slot] = (j, i)
            slot += 1
    return line, over, max(len(line), slot)


def exchange(
    n, t, x_ref, oc_ref, vc_ref, ret_ref, pv_ref, po_ref, wv_ref, wo_ref, fv_ref, sv_ref, fo_ref, so_ref,
    copy_v, copy_o, step_v, step_o, nfv, nsv, nfo, nso,
    wall, flip, own, pall, xin, cot, old, pr, gsend, grecv, gpart, gfin, total, dall, dir32, dirs, sq, scales,
    load_sem, p_send, p_recv, x_send, x_recv, core_send, core_recv, g_send, g_recv, f_send, f_recv,
    d_send, d_recv, q_send, q_recv, up_send, down_send, over_send, w_recv,
):
    me = lax.axis_index("fs")
    tp = lax.axis_index("tp")
    core = lax.rem(tp, 2)
    partner = tp + 1 - 2 * core
    x = tp // 2
    z, y = me // 2, lax.rem(me, 2)
    levels = n // 2
    across = me + 1 - 2 * y
    q, columns = wv_ref.shape
    rows = 2 * q
    rr, rank = fv_ref.shape[0], pv_ref.shape[1]
    count, early = cut(rows)
    size = rows // count
    ways = share(q, t)
    part_rows = q // ways
    streamed = levels <= STREAMED
    paired = levels == 4 and 4 * q % LANES == 0
    base = (q, 0)

    def remote(src, dst, ssem, rsem, device):
        return pltpu.make_async_remote_copy(
            src_ref=src, dst_ref=dst, send_sem=ssem, recv_sem=rsem,
            device_id=device, device_id_type=pl.DeviceIdType.MESH,
        )

    barrier = pltpu.get_barrier_semaphore()
    for d in range(1, n):
        pl.semaphore_signal(
            barrier, inc=1, device_id={"fs": lax.rem(me + d, n)}, device_id_type=pl.DeviceIdType.MESH
        )
    for d in range(1, t):
        pl.semaphore_signal(
            barrier, inc=1, device_id={"tp": lax.rem(tp + d, t)}, device_id_type=pl.DeviceIdType.MESH
        )

    @pl.when(core == 0)
    def _():
        pltpu.make_async_copy(pv_ref, pall.at[0, me], load_sem.at[0]).start()

    @pl.when(core == 1)
    def _():
        pltpu.make_async_copy(po_ref, pall.at[1, me], load_sem.at[0]).start()

    def load(src, dst, k):
        copy = pltpu.make_async_copy(src, dst, load_sem.at[k])
        copy.start()
        return copy

    weights = [load(wv_ref, own.at[0], 1), load(wo_ref, own.at[1], 2)]

    @pl.when(core == 0)
    def _():
        pltpu.make_async_copy(x_ref, xin, load_sem.at[3]).start()

    @pl.when(core == 1)
    def _():
        pltpu.make_async_copy(oc_ref, xin, load_sem.at[3]).start()

    cots = [load(vc_ref, cot.at[0], 4), load(ret_ref, cot.at[1], 5)]
    olds = [load(ref, old.at[k], 6 + k) for k, ref in enumerate((fv_ref, sv_ref, fo_ref, so_ref))]

    pltpu.make_async_copy(pv_ref, pall.at[core, me], load_sem.at[0]).wait()
    pl.semaphore_wait(barrier, n - 1 + t - 1)

    sends = []

    def go(copy):
        copy.start()
        sends.append(copy)
        return copy

    def spread(place, ssem, rsem):
        mine = place(me)
        first = [go(remote(mine, mine, ssem.at[0], rsem.at[0], {"fs": across}))]
        for d in range(1, levels):
            target = lax.rem(z + d, levels) * 2 + y
            first.append(go(remote(mine, mine, ssem.at[d], rsem.at[d], {"fs": target})))
        return first

    def pass_on(first, place, ssem, rsem):
        second = []
        for d in range(1, levels):
            first[d].wait_recv()
            block = place(lax.rem(z + levels - d, levels) * 2 + y)
            second.append(
                go(remote(block, block, ssem.at[levels + d], rsem.at[levels + d], {"fs": across}))
            )
        return first[:1] + second

    line, over, slots = schedule(levels, count, early)

    def piece(level, side, i):
        column = y if side == 0 else 1 - y
        return wall.at[level * 2 + column, pl.ds(i * size, size)]

    def along(slot, step):
        side, s, i = line[slot]
        level = z - s if step > 0 else z + s
        place = piece(level, side, i)
        ssem = (up_send if step > 0 else down_send).at[slot % DEEP]
        return remote(place, place, ssem, w_recv.at[side, level, i], {"fs": (z + step) * 2 + y})

    def goes(slot, step):
        s = line[slot][1]
        if step > 0:
            return jnp.logical_and(z >= s, z < levels - 1)
        return jnp.logical_and(z + s < levels, z > 0)

    def nearest(j):
        if j == 0:
            return z
        low = jnp.minimum(z, levels - 1 - z)
        near = z + (j + 1) // 2 * (1 if j % 2 else -1)
        far = jnp.where(z < levels - 1 - z, j, levels - 1 - j)
        return jnp.where(j <= 2 * low, near, far)

    def crossing(slot):
        j, i = over[slot]
        level = nearest(j)
        place = piece(level, 0, i)
        return remote(place, place, over_send.at[slot % DEPTH], w_recv.at[1, level, i], {"fs": across})

    held = set()

    def landed(side, level, i):
        place = piece(level, side, i)
        remote(place, place, over_send.at[0], w_recv.at[side, level, i], {"fs": across}).wait_recv()

    def ensure(side, k, i):
        if (side, k, i) in held:
            return
        held.add((side, k, i))
        if k == 0:
            landed(side, z, i)
            return

        @pl.when(z >= k)
        def _():
            landed(side, z - k, i)

        @pl.when(z + k < levels)
        def _():
            landed(side, z + k, i)

    def crossed(j, i):
        if ("over", j, i) not in held:
            held.add(("over", j, i))
            landed(1, nearest(j), i)

    def tight(step):
        return z + step == (levels - 1 if step > 0 else 0)

    def drained(slot):
        for depth in (DEPTH, DEEP):
            if 0 <= slot - depth < len(line):
                for step in (1, -1):
                    close = tight(step) if depth == DEPTH else jnp.logical_not(tight(step))

                    @pl.when(jnp.logical_and(goes(slot - depth, step), close))
                    def _():
                        along(slot - depth, step).wait_send()
        if slot - DEPTH in over:
            crossing(slot - DEPTH).wait_send()

    def advance(slot):
        drained(slot)
        if slot < len(line):
            side, s, i = line[slot]
            if side == 1 or s > 0:
                ensure(side, s, i)
            for step in (1, -1):
                @pl.when(goes(slot, step))
                def _():
                    along(slot, step).start()
        if slot in over:
            j, i = over[slot]
            for k in range(1, j + 1):
                ensure(0, k, i)
            crossing(slot).start()

    steps = (step_v, step_o)

    def keep(block, side, low, high, value):
        if side == 0:
            copy_v[block, low:high] = value.astype(BF16)
        else:
            flip[block, low:high] = value.astype(BF16)

    def turn(chunk):
        start = pl.multiple_of(chunk * LANES, LANES)
        tile = flip.reshape(n * q, columns)[pl.ds(start, LANES)]
        copy_o[:, pl.ds(start, LANES)] = tile.astype(F32).T.astype(BF16)

    def moved(block, side, low, high):
        part = jnp.dot(pall[side, block, low:high], dirs[side], preferred_element_type=F32)
        return part * scales[side, 0:1, 0:1]

    def renew(block, side, low, high):
        old_part = wall[block, base[side] + low:base[side] + high].astype(F32)
        keep(block, side, low, high, old_part + moved(block, side, low, high))

    def renew_own(side):
        step = moved(me, side, 0, q)
        steps[side][...] = step
        keep(me, side, 0, q, own[side] + step)

    def unit(side, j, half, low, high):
        if side == 0 and j == 0:
            renew_own(half)
            return
        for i in range((base[half] + low) // size, -(-(base[half] + high) // size)):
            if side == 1 and (i < count - early or j == 0):
                if i < count - early:
                    crossed(j, i)
                else:
                    ensure(1, 0, i)
            else:
                for k in range(1, j + 1):
                    ensure(side, k, i)
        renew(nearest(j) * 2 + (y if side == 0 else 1 - y), half, low, high)

    def plan():
        at_line = {item: slot for slot, item in enumerate(line)}
        at_over = {item: slot for slot, item in over.items()}
        units, flipped = [], [0] * levels

        def add(ready, work, *args):
            units.append((ready, len(units), work, args))

        for j in range(levels):
            for half in (1, 0):
                for side in (0, 1):
                    fine = 2 * size if j == levels - 1 and q % (2 * size) == 0 else q
                    for low in range(0, q, fine):
                        ready, start = 0, base[half] + low
                        for i in range(start // size, -(-(start + fine) // size)):
                            if side == 1 and (j == 0 or i < count - early):
                                ready = max(ready, at_over[j, i] + LAG)
                            elif j > 0:
                                ready = max(ready, at_line[side, j - 1, i] + LAG)
                        if half == 1:
                            flipped[j] = max(flipped[j], ready)
                        add(ready, unit, side, j, half, low, low + fine)
            if paired and j >= 2:
                group = 4 * q // LANES
                near = z // 2
                low = jnp.where(z < 2, 0, 1)
                split = 2 * q // LANES
                rest = group - split
                if j == 2:
                    for c in range(group):
                        add(max(flipped[:3]), turn, near * group + c)
                    for c in range(split):
                        add(max(flipped[:3]), turn, (1 - near) * group + low * rest + c)
                else:
                    for c in range(rest):
                        add(max(flipped), turn, (1 - near) * group + (1 - low) * split + c)
        return sorted(units, key=lambda item: item[:2])

    chain = {}

    def part(block):
        return pall.at[core, block, pl.ds(x * part_rows, part_rows)]

    def shared(block):
        for d in range(1, ways):
            place = part(block)
            target = lax.rem(x + d, ways) * 2 + core
            chain["shared"].append(
                go(remote(place, place, x_send.at[d, block], x_recv.at[d, block], {"tp": target}))
            )

    def hook_pass():
        first = chain["proj"]
        second = pass_on(first, part, p_send, p_recv)
        for d in range(1, levels):
            shared(lax.rem(z + levels - d, levels) * 2 + y)
        chain["proj"] = second

    def hook_share():
        second = chain["proj"]
        for d, copy in enumerate(second):
            copy.wait_recv()
            shared(lax.rem(z + levels - d, levels) * 2 + 1 - y)

    def hook_grads():
        for copy in chain["shared"]:
            copy.wait_recv()
        chain["whole"] = go(
            remote(pall.at[core], pall.at[core], core_send.at[0], core_recv.at[0], {"tp": partner})
        )
        pltpu.make_async_copy(x_ref, xin, load_sem.at[3]).wait()
        pr[core] = jnp.dot(xin[...], flat(pall[core]), preferred_element_type=F32).astype(BF16)
        swapped = go(remote(pr.at[core], pr.at[core], core_send.at[1], core_recv.at[1], {"tp": partner}))
        for copy in cots:
            copy.wait()
        swapped.wait_recv()
        for side in (0, 1):
            grad = lax.dot_general(
                pr[side], cot[side], (((0,), (0,)), ((), ())), preferred_element_type=F32
            )
            for peer in range(n):
                gsend[peer // 2, peer % 2, :, side * columns:(side + 1) * columns] = (
                    grad[peer * rr:(peer + 1) * rr].astype(BF16)
                )
        for d in range(1, levels):
            scatter(d, "start")
        final(ends, gsend.at[z, 1 - y], 0, across, "start")

    inside = jnp.logical_and(z > 0, z < levels - 1) if levels > 3 else z >= 0
    ends = jnp.logical_not(inside)

    def scatter(d, act):
        level = lax.rem(z + d, levels)

        def send(kind, owner):
            copy = remote(
                gsend.at[level], grecv.at[kind, z], g_send.at[d], g_recv.at[kind, z], {"fs": owner * 2 + y}
            )
            copy.start() if act == "start" else copy.wait_send()

        if levels < 4:
            send(0, level)
            return
        inner = jnp.logical_and(level > 0, level < levels - 1)
        owner = jnp.where(level == 0, 1, levels - 2)

        @pl.when(inner)
        def _():
            send(0, level)

        @pl.when(jnp.logical_and(jnp.logical_not(inner), z != owner))
        def _():
            send(1, owner)

    def final(when, src, k, peer, act):
        @pl.when(when)
        def _():
            copy = remote(src, gfin.at[k], f_send.at[k], f_recv.at[k], {"fs": peer})
            copy.start() if act == "start" else copy.wait_send()

    def arrived(kind, d):
        level = lax.rem(z + d, levels)
        place = grecv.at[kind, level]
        remote(place, place, g_send.at[d], g_recv.at[kind, level], {"fs": across}).wait_recv()
        return place[...].astype(F32)

    def finals(act):
        final(inside, gpart.at[0, 1 - y], 0, across, act)
        if levels > 3:
            for own_level, end in ((1, 0), (levels - 2, levels - 1)):
                final(z == own_level, gpart.at[1, y], 1, end * 2 + y, act)
                final(z == own_level, gpart.at[1, 1 - y], 2, end * 2 + 1 - y, act)

    def hook_partial():
        @pl.when(inside)
        def _():
            summed = gsend[z].astype(F32)
            for d in range(1, levels):
                summed += arrived(0, d)
            gpart[0] = summed.astype(BF16)

        if levels > 3:
            for own_level, end, sources in (
                (1, 0, range(1, levels - 1)), (levels - 2, levels - 1, range(2, levels))
            ):
                @pl.when(z == own_level)
                def _():
                    summed = gsend[end].astype(F32)
                    for d in sources:
                        summed += arrived(1, d)
                    gpart[1] = summed.astype(BF16)

        finals("start")

    def hook_moments():
        for copy in olds:
            copy.wait()

        def fetched(k):
            remote(gfin.at[k], gfin.at[k], f_send.at[k], f_recv.at[k], {"fs": across}).wait_recv()
            return gfin[k].astype(F32)

        @pl.when(inside)
        def _():
            total[...] = gpart[0, y].astype(F32) + fetched(0)

        if levels > 3:
            @pl.when(ends)
            def _():
                total[...] = gsend[z, y].astype(F32) + fetched(0) + fetched(1) + fetched(2)

        for side, refs in ((0, (nfv, nsv)), (1, (nfo, nso))):
            grad = total[:, side * columns:(side + 1) * columns]
            new_first, new_second, direction = adapt(old[2 * side], old[2 * side + 1], grad)
            refs[0][...] = new_first
            refs[1][...] = new_second
            dall[me, :, side * columns:(side + 1) * columns] = direction
        chain["dirs"] = spread(lambda block: dall.at[block], d_send, d_recv)

    def hook_dirs():
        chain["dirs"] = pass_on(chain["dirs"], lambda block: dall.at[block], d_send, d_recv)

    def hook_sums():
        for copy in chain["dirs"]:
            copy.wait_recv()
        sums = []
        for side in (0, 1):
            for k in range(n):
                dir32[k * rr:(k + 1) * rr] = dall[k, :, side * columns:(side + 1) * columns].astype(F32)
            whole = dir32[...]
            sums.append(jnp.sum(jnp.square(whole)))
            dirs[side] = whole.astype(BF16)
        row = lax.broadcasted_iota(jnp.int32, sq.shape[1:], 0)
        sq[tp] = jnp.where(row == 0, sums[0], sums[1])
        chain["sq"] = [
            go(remote(sq.at[tp], sq.at[tp], q_send.at[d], q_recv.at[d], {"tp": lax.rem(tp + d, t)}))
            for d in range(1, t)
        ]

    def hook_scales():
        for copy in chain["sq"]:
            copy.wait_recv()
        chain["whole"].wait_recv()
        totals = jnp.sum(sq[...], axis=0)
        spread_scales = lax.rsqrt(totals / float(rank * columns * t) + norm_eps)
        for side in (0, 1):
            scales[side] = jnp.broadcast_to(spread_scales[side:side + 1], scales.shape[1:])

    hooks = dict(zip(HOOKS, (
        hook_pass, hook_share, hook_grads, hook_partial, hook_moments, hook_dirs, hook_sums, hook_scales
    )))
    chain["shared"] = []
    chain["proj"] = spread(part, p_send, p_recv)
    for side in (0, 1):
        weights[side].wait()
        wall[me, base[side]:base[side] + q] = own[side].astype(BF16)
    units = plan() if streamed else []
    end = max(slots, max(HOOKS) + 1)
    for slot in range(end):
        if slot in hooks:
            hooks[slot]()
        advance(slot)
        if slot >= max(HOOKS):
            for _ in range(UNITS):
                if units and units[0][0] <= slot:
                    _, _, work, args = units.pop(0)
                    work(*args)
    for _, _, work, args in units:
        work(*args)
    for slot in range(end, slots + DEEP):
        drained(slot)

    for k in range(1, levels):
        for i in range(count):
            ensure(0, k, i)
        for i in range(count - early, count):
            ensure(1, k, i)
    for i in range(count - early, count):
        ensure(1, 0, i)
    for j in range(levels):
        for i in range(count - early):
            crossed(j, i)
    if not streamed:
        def whole_block(block, carry):
            for side in (0, 1):
                renew(block, side, 0, q)
            return carry

        lax.fori_loop(0, n, whole_block, 0)
        for side in (0, 1):
            renew_own(side)
    if not (streamed and paired):
        def one_chunk(chunk, carry):
            turn(chunk)
            return carry

        lax.fori_loop(0, n * q // LANES, one_chunk, 0)
    for copy in sends:
        copy.wait_send()
    for d in range(1, levels):
        scatter(d, "wait")
    final(ends, gsend.at[z, 1 - y], 0, across, "wait")
    finals("wait")


def finish(*refs):
    sem, count = refs[-1], len(refs) // 2
    copies = []
    for src, dst in zip(refs[:count], refs[count:]):
        rows = src.shape[0]
        parts = SPLIT if rows % (16 * SPLIT) == 0 else 1
        for p in range(parts):
            place = pl.ds(p * (rows // parts), rows // parts)
            copies.append(pltpu.make_async_copy(src.at[place], dst.at[place], sem.at[len(copies)]))
    for copy in copies:
        copy.start()
    for copy in copies:
        copy.wait()


def per_device(
    n, t,
    inputs, value_cot, retained, output_cot, proj_value, proj_output, w_value, w_output,
    first_value, second_value, first_output, second_output,
):
    tokens, width = inputs.shape
    q, rank = proj_value.shape
    columns = value_cot.shape[1]
    rr = first_value.shape[0]
    levels = n // 2
    pieces, _ = cut(2 * q)
    ways = share(q, t)
    hbm = pl.BlockSpec(memory_space=pltpu.HBM)
    vmem = pl.BlockSpec(memory_space=pltpu.VMEM)
    anywhere = pl.BlockSpec(memory_space=pl.ANY)
    dma = pltpu.SemaphoreType.DMA
    results = pl.pallas_call(
        functools.partial(exchange, n, t),
        out_shape=(
            pltpu.VMEM((n, q, columns), BF16),
            pltpu.VMEM((columns, n * q), BF16),
            pltpu.VMEM((q, columns), F32),
            pltpu.VMEM((q, columns), F32),
            pltpu.VMEM((rr, columns), F32),
            pltpu.VMEM((rr, columns), F32),
            pltpu.VMEM((rr, columns), F32),
            pltpu.VMEM((rr, columns), F32),
        ),
        in_specs=[hbm] * 12,
        out_specs=(vmem,) * 8,
        scratch_shapes=[
            pltpu.VMEM((n, 2 * q, columns), BF16),
            pltpu.VMEM((n, q, columns), BF16),
            pltpu.VMEM((2, q, columns), F32),
            pltpu.VMEM((2, n, q, rank), BF16),
            pltpu.VMEM((tokens, width), BF16),
            pltpu.VMEM((2, tokens, columns), BF16),
            pltpu.VMEM((4, rr, columns), F32),
            pltpu.VMEM((2, tokens, rank), BF16),
            pltpu.VMEM((levels, 2, rr, 2 * columns), BF16),
            pltpu.VMEM((2, levels, 2, rr, 2 * columns), BF16),
            pltpu.VMEM((2, 2, rr, 2 * columns), BF16),
            pltpu.VMEM((3, rr, 2 * columns), BF16),
            pltpu.VMEM((rr, 2 * columns), F32),
            pltpu.VMEM((n, rr, 2 * columns), BF16),
            pltpu.VMEM((rank, columns), F32),
            pltpu.VMEM((2, rank, columns), BF16),
            pltpu.VMEM((t, 8, 128), F32),
            pltpu.VMEM((2, 8, 128), F32),
            dma((10,)), dma((n,)), dma((n,)), dma((ways, n)), dma((ways, n)), dma((2,)), dma((2,)),
            dma((levels,)), dma((2, levels)), dma((3,)), dma((3,)), dma((n,)), dma((n,)),
            dma((t,)), dma((t,)),
            dma((DEEP,)), dma((DEEP,)), dma((DEPTH,)), dma((2, levels, pieces)),
        ],
        compiler_params=pltpu.CompilerParams(
            collective_id=0, has_side_effects=True, vmem_limit_bytes=51 * 1024 * 1024
        ),
        name="exchange",
    )(
        inputs, output_cot, value_cot, retained, proj_value, proj_output, w_value, w_output.T,
        first_value, second_value, first_output, second_output,
    )
    full = n * q
    values = (results[0].reshape(full, columns),) + tuple(results[1:])
    copy_v, copy_o, step_v, step_o, first_v, second_v, first_o, second_o = pl.pallas_call(
        finish,
        out_shape=tuple(jax.ShapeDtypeStruct(value.shape, value.dtype) for value in values),
        in_specs=[anywhere] * 8,
        out_specs=(anywhere,) * 8,
        scratch_shapes=[dma((8 * SPLIT,))],
        compiler_params=pltpu.CompilerParams(vmem_limit_bytes=12 * 1024 * 1024),
        name="finish",
    )(*values)
    return (step_v, step_o.T, copy_v, copy_o, first_v, second_v, first_o, second_o)


def solution(mesh):
    in_specs = (
        P("fs", None),
        P("fs", "tp"),
        P("fs", "tp"),
        P("fs", None),
        P("fs", None),
        P("fs", None),
        P("fs", "tp"),
        P("tp", "fs"),
        P("fs", "tp"),
        P("fs", "tp"),
        P("fs", "tp"),
        P("fs", "tp"),
    )
    out_specs = (
        P("fs", "tp"),
        P("tp", "fs"),
        P(None, "tp"),
        P("tp", None),
        P("fs", "tp"),
        P("fs", "tp"),
        P("fs", "tp"),
        P("fs", "tp"),
    )
    return jax.shard_map(
        functools.partial(per_device, mesh.shape["fs"], mesh.shape["tp"]),
        mesh=mesh, in_specs=in_specs, out_specs=out_specs, check_vma=False,
    )
```

```python
import functools

import jax
import jax.numpy as jnp
from jax import lax
from jax.experimental import pallas as pl
from jax.experimental.pallas import tpu as pltpu
from jax.sharding import PartitionSpec as P

BF16 = jnp.bfloat16
F32 = jnp.float32

beta_one = 0.8
beta_two = 0.9
moment_eps = 1e-08
norm_eps = 1e-06

PIECES = 12
SHARE = 0.2
DEPTH = 5
HOOKS = (2, 5, 11, 12, 13, 20, 25, 31, 36)
LAG = 3
UNITS = 4
LANES = 128
DEEP = 12
LATE = 1
SPLIT = 2
STREAMED = 8


def adapt(first, second, grad):
    new_first = beta_one * first + (1.0 - beta_one) * grad
    new_second = beta_two * second + (1.0 - beta_two) * grad * grad
    direction = (new_first / (jnp.sqrt(new_second) + moment_eps)).astype(BF16)
    return (new_first, new_second, direction)


def flat(block):
    parts, rows, columns = block.shape
    if rows % 16 == 0:
        return block.reshape(parts * rows, columns)
    return block.astype(F32).reshape(parts * rows, columns).astype(block.dtype)


def cut(rows):
    if rows % (16 * PIECES) == 0:
        ahead = max(32, int(rows * SHARE) // 16 * 16)
        late, size = rows - ahead, rows // PIECES
        return list(range(0, late, size)) + [late, late + ahead // 32 * 16, rows], 2
    edges = list(range(0, rows + 1, 16))
    return edges, max(1, int((len(edges) - 1) * SHARE))


def share(q, t):
    ways = t // 2
    return ways if q % (16 * ways) == 0 else 1


def schedule(levels, count, early):
    line, sent = [], {}
    for s in range(levels - 1):
        for i in range(count):
            sent[s + 1, i] = len(line)
            line.append((0, s, i))
        for i in range(count - early, count):
            line.append((1, s, i))
    over = {}
    slot = 0
    for i in list(range(count - early, count)) + list(range(count - early)):
        over[slot] = (0, i)
        slot += 1
    for j in range(1, levels):
        for i in range(count - early):
            slot = max(slot, sent[j, i] + 3)
            over[slot] = (j, i)
            slot += 1
    return line, over, max(len(line), slot)


def exchange(
    n, t, x_ref, oc_ref, vc_ref, ret_ref, pv_ref, po_ref, wv_ref, wo_ref, fv_ref, sv_ref, fo_ref, so_ref,
    copy_v, copy_o, step_v, step_o, nfv, nsv, nfo, nso,
    wall, flip, own, pall, xin, cot, old, pr, gsend, grecv, gpart, gfin, total, dall, dir32, dirs, sq, fsq, scales,
    load_sem, p_send, p_recv, x_send, x_recv, core_send, core_recv, g_send, g_recv, f_send, f_recv,
    d_send, d_recv, q_send, q_recv, s_send, s_recv, up_send, down_send, over_send, w_recv,
):
    me = lax.axis_index("fs")
    tp = lax.axis_index("tp")
    core = lax.rem(tp, 2)
    partner = tp + 1 - 2 * core
    x = tp // 2
    z, y = me // 2, lax.rem(me, 2)
    levels = n // 2
    across = me + 1 - 2 * y
    q, columns = wv_ref.shape
    rows = 2 * q
    rr, rank = fv_ref.shape[0], pv_ref.shape[1]
    edges, early = cut(rows)
    count = len(edges) - 1
    size = edges[1]
    ways = share(q, t)
    part_rows = q // ways
    streamed = levels <= STREAMED
    paired = levels == 4 and 4 * q % LANES == 0
    base = (q, 0)

    def remote(src, dst, ssem, rsem, device):
        return pltpu.make_async_remote_copy(
            src_ref=src, dst_ref=dst, send_sem=ssem, recv_sem=rsem,
            device_id=device, device_id_type=pl.DeviceIdType.MESH,
        )

    barrier = pltpu.get_barrier_semaphore()
    for d in range(1, n):
        pl.semaphore_signal(
            barrier, inc=1, device_id={"fs": lax.rem(me + d, n)}, device_id_type=pl.DeviceIdType.MESH
        )
    for d in range(1, t):
        pl.semaphore_signal(
            barrier, inc=1, device_id={"tp": lax.rem(tp + d, t)}, device_id_type=pl.DeviceIdType.MESH
        )

    @pl.when(core == 0)
    def _():
        pltpu.make_async_copy(pv_ref, pall.at[0, me], load_sem.at[0]).start()

    @pl.when(core == 1)
    def _():
        pltpu.make_async_copy(po_ref, pall.at[1, me], load_sem.at[0]).start()

    def load(src, dst, k):
        copy = pltpu.make_async_copy(src, dst, load_sem.at[k])
        copy.start()
        return copy

    weights = [load(wv_ref, own.at[0], 1), load(wo_ref, own.at[1], 2)]

    @pl.when(core == 0)
    def _():
        pltpu.make_async_copy(x_ref, xin, load_sem.at[3]).start()

    @pl.when(core == 1)
    def _():
        pltpu.make_async_copy(oc_ref, xin, load_sem.at[3]).start()

    cots = [load(vc_ref, cot.at[0], 4), load(ret_ref, cot.at[1], 5)]
    olds = [load(ref, old.at[k], 6 + k) for k, ref in enumerate((fv_ref, sv_ref, fo_ref, so_ref))]

    pltpu.make_async_copy(pv_ref, pall.at[core, me], load_sem.at[0]).wait()
    pl.semaphore_wait(barrier, n - 1 + t - 1)

    sends = []

    def go(copy):
        copy.start()
        sends.append(copy)
        return copy

    def spread(place, ssem, rsem):
        mine = place(me)
        first = [go(remote(mine, mine, ssem.at[0], rsem.at[0], {"fs": across}))]
        for d in range(1, levels):
            target = lax.rem(z + d, levels) * 2 + y
            first.append(go(remote(mine, mine, ssem.at[d], rsem.at[d], {"fs": target})))
        return first

    def pass_on(first, place, ssem, rsem):
        second = []
        for d in range(1, levels):
            first[d].wait_recv()
            block = place(lax.rem(z + levels - d, levels) * 2 + y)
            second.append(
                go(remote(block, block, ssem.at[levels + d], rsem.at[levels + d], {"fs": across}))
            )
        return first[:1] + second

    line, over, slots = schedule(levels, count, early)

    def piece(level, side, i):
        column = y if side == 0 else 1 - y
        return wall.at[level * 2 + column, pl.ds(edges[i], edges[i + 1] - edges[i])]

    def along(slot, step):
        side, s, i = line[slot]
        level = z - s if step > 0 else z + s
        place = piece(level, side, i)
        ssem = (up_send if step > 0 else down_send).at[slot % DEEP]
        return remote(place, place, ssem, w_recv.at[side, level, i], {"fs": (z + step) * 2 + y})

    def goes(slot, step):
        s = line[slot][1]
        if step > 0:
            return jnp.logical_and(z >= s, z < levels - 1)
        return jnp.logical_and(z + s < levels, z > 0)

    def nearest(j):
        if j == 0:
            return z
        low = jnp.minimum(z, levels - 1 - z)
        near = z + (j + 1) // 2 * (1 if j % 2 else -1)
        far = jnp.where(z < levels - 1 - z, j, levels - 1 - j)
        return jnp.where(j <= 2 * low, near, far)

    def crossing(slot):
        j, i = over[slot]
        level = nearest(j)
        place = piece(level, 0, i)
        return remote(place, place, over_send.at[slot % DEPTH], w_recv.at[1, level, i], {"fs": across})

    held = set()

    def covering(start, stop):
        return [i for i in range(count) if edges[i] < stop and edges[i + 1] > start]

    def landed(side, level, i):
        place = piece(level, side, i)
        remote(place, place, over_send.at[0], w_recv.at[side, level, i], {"fs": across}).wait_recv()

    def ensure(side, k, i):
        if (side, k, i) in held:
            return
        held.add((side, k, i))
        if k == 0:
            landed(side, z, i)
            return

        @pl.when(z >= k)
        def _():
            landed(side, z - k, i)

        @pl.when(z + k < levels)
        def _():
            landed(side, z + k, i)

    def crossed(j, i):
        if ("over", j, i) not in held:
            held.add(("over", j, i))
            landed(1, nearest(j), i)

    def tight(step):
        return z + step == (levels - 1 if step > 0 else 0)

    done = {"tight": 0, "loose": 0, "over": 0}

    def drained(close, loose):
        for kind, limit in (("tight", close), ("loose", loose)):
            for slot in range(done[kind], min(limit, len(line))):
                for step in (1, -1):
                    paced = tight(step) if kind == "tight" else jnp.logical_not(tight(step))

                    @pl.when(jnp.logical_and(goes(slot, step), paced))
                    def _():
                        along(slot, step).wait_send()
            done[kind] = max(done[kind], limit)
        for slot in range(done["over"], close):
            if slot in over:
                crossing(slot).wait_send()
        done["over"] = max(done["over"], close)

    def advance(slot):
        drained(slot - DEPTH + 1, slot - DEEP + 1)
        if slot < len(line):
            side, s, i = line[slot]
            if side == 1 or s > 0:
                ensure(side, s, i)
            for step in (1, -1):
                @pl.when(jnp.logical_and(goes(slot, step), tight(step)))
                def _():
                    along(slot, step).start()
        if 0 <= slot - LATE < len(line):
            for step in (1, -1):
                @pl.when(jnp.logical_and(goes(slot - LATE, step), jnp.logical_not(tight(step))))
                def _():
                    along(slot - LATE, step).start()
        if slot in over:
            j, i = over[slot]
            for k in range(1, j + 1):
                ensure(0, k, i)
            crossing(slot).start()

    steps = (step_v, step_o)

    def keep(block, side, low, high, value):
        if side == 0:
            copy_v[block, low:high] = value.astype(BF16)
        else:
            flip[block, low:high] = value.astype(BF16)

    def turn(chunk):
        start = pl.multiple_of(chunk * LANES, LANES)
        tile = flip.reshape(n * q, columns)[pl.ds(start, LANES)]
        copy_o[:, pl.ds(start, LANES)] = tile.astype(F32).T.astype(BF16)

    def moved(block, side, low, high):
        part = jnp.dot(pall[side, block, low:high], dirs[side], preferred_element_type=F32)
        return part * scales[side, 0:1, 0:1]

    def renew(block, side, low, high):
        old_part = wall[block, base[side] + low:base[side] + high].astype(F32)
        keep(block, side, low, high, old_part + moved(block, side, low, high))

    def renew_own(side):
        step = moved(me, side, 0, q)
        steps[side][...] = step
        keep(me, side, 0, q, own[side] + step)

    def unit(side, j, half, low, high):
        if side == 0 and j == 0:
            renew_own(half)
            return
        for i in covering(base[half] + low, base[half] + high):
            if side == 1 and (i < count - early or j == 0):
                if i < count - early:
                    crossed(j, i)
                else:
                    ensure(1, 0, i)
            else:
                for k in range(1, j + 1):
                    ensure(side, k, i)
        renew(nearest(j) * 2 + (y if side == 0 else 1 - y), half, low, high)

    def plan():
        at_line = {item: slot for slot, item in enumerate(line)}
        at_over = {item: slot for slot, item in over.items()}
        units, flipped = [], [0] * levels

        def add(ready, work, *args):
            units.append((ready, len(units), work, args))

        for j in range(levels):
            for half in (1, 0):
                for side in (0, 1):
                    fine = 2 * size if j == levels - 1 and q % (2 * size) == 0 else q
                    for low in range(0, q, fine):
                        ready, start = 0, base[half] + low
                        for i in covering(start, start + fine):
                            if side == 1 and (j == 0 or i < count - early):
                                ready = max(ready, at_over[j, i] + LAG)
                            elif j > 0:
                                ready = max(ready, at_line[side, j - 1, i] + LAG)
                        if half == 1:
                            flipped[j] = max(flipped[j], ready)
                        add(ready, unit, side, j, half, low, low + fine)
            if paired and j >= 2:
                group = 4 * q // LANES
                near = z // 2
                low = jnp.where(z < 2, 0, 1)
                split = 2 * q // LANES
                rest = group - split
                if j == 2:
                    for c in range(group):
                        add(max(flipped[:3]), turn, near * group + c)
                    for c in range(split):
                        add(max(flipped[:3]), turn, (1 - near) * group + low * rest + c)
                else:
                    for c in range(rest):
                        add(max(flipped), turn, (1 - near) * group + (1 - low) * split + c)
        return sorted(units, key=lambda item: item[:2])

    chain = {}

    def part(block):
        return pall.at[core, block, pl.ds(x * part_rows, part_rows)]

    def shared(block):
        for d in range(1, ways):
            place = part(block)
            target = lax.rem(x + d, ways) * 2 + core
            chain["shared"].append(
                go(remote(place, place, x_send.at[d, block], x_recv.at[d, block], {"tp": target}))
            )

    def hook_pass():
        first = chain["proj"]
        second = pass_on(first, part, p_send, p_recv)
        for d in range(1, levels):
            shared(lax.rem(z + levels - d, levels) * 2 + y)
        chain["proj"] = second

    def hook_share():
        second = chain["proj"]
        for d, copy in enumerate(second):
            copy.wait_recv()
            shared(lax.rem(z + levels - d, levels) * 2 + 1 - y)

    def hook_grads():
        for copy in chain["shared"]:
            copy.wait_recv()
        chain["whole"] = go(
            remote(pall.at[core], pall.at[core], core_send.at[0], core_recv.at[0], {"tp": partner})
        )
        pltpu.make_async_copy(x_ref, xin, load_sem.at[3]).wait()
        pr[core] = jnp.dot(xin[...], flat(pall[core]), preferred_element_type=F32).astype(BF16)
        chain["swap"] = go(
            remote(pr.at[core], pr.at[core], core_send.at[1], core_recv.at[1], {"tp": partner})
        )

    def project(side):
        grad = lax.dot_general(
            pr[side], cot[side], (((0,), (0,)), ((), ())), preferred_element_type=F32
        )
        for peer in range(n):
            gsend[peer // 2, peer % 2, :, side * columns:(side + 1) * columns] = (
                grad[peer * rr:(peer + 1) * rr].astype(BF16)
            )

    def hook_first():
        for copy in cots:
            copy.wait()
        chain["swap"].wait_recv()
        project(0)

    def hook_second():
        project(1)
        for d in range(1, levels):
            scatter(d, "start")
        final(ends, gsend.at[z, 1 - y], 0, across, "start")

    inside = jnp.logical_and(z > 0, z < levels - 1) if levels > 3 else z >= 0
    ends = jnp.logical_not(inside)

    def scatter(d, act):
        level = lax.rem(z + d, levels)

        def send(kind, owner):
            copy = remote(
                gsend.at[level], grecv.at[kind, z], g_send.at[d], g_recv.at[kind, z], {"fs": owner * 2 + y}
            )
            copy.start() if act == "start" else copy.wait_send()

        if levels < 4:
            send(0, level)
            return
        inner = jnp.logical_and(level > 0, level < levels - 1)
        owner = jnp.where(level == 0, 1, levels - 2)

        @pl.when(inner)
        def _():
            send(0, level)

        @pl.when(jnp.logical_and(jnp.logical_not(inner), z != owner))
        def _():
            send(1, owner)

    def final(when, src, k, peer, act):
        @pl.when(when)
        def _():
            copy = remote(src, gfin.at[k], f_send.at[k], f_recv.at[k], {"fs": peer})
            copy.start() if act == "start" else copy.wait_send()

    def arrived(kind, d):
        level = lax.rem(z + d, levels)
        place = grecv.at[kind, level]
        remote(place, place, g_send.at[d], g_recv.at[kind, level], {"fs": across}).wait_recv()
        return place[...].astype(F32)

    def finals(act):
        final(inside, gpart.at[0, 1 - y], 0, across, act)
        if levels > 3:
            for own_level, end in ((1, 0), (levels - 2, levels - 1)):
                final(z == own_level, gpart.at[1, y], 1, end * 2 + y, act)
                final(z == own_level, gpart.at[1, 1 - y], 2, end * 2 + 1 - y, act)

    def hook_partial():
        @pl.when(inside)
        def _():
            summed = gsend[z].astype(F32)
            for d in range(1, levels):
                summed += arrived(0, d)
            gpart[0] = summed.astype(BF16)

        if levels > 3:
            for own_level, end, sources in (
                (1, 0, range(1, levels - 1)), (levels - 2, levels - 1, range(2, levels))
            ):
                @pl.when(z == own_level)
                def _():
                    summed = gsend[end].astype(F32)
                    for d in sources:
                        summed += arrived(1, d)
                    gpart[1] = summed.astype(BF16)

        finals("start")

    def hook_moments():
        for copy in olds:
            copy.wait()

        def fetched(k):
            remote(gfin.at[k], gfin.at[k], f_send.at[k], f_recv.at[k], {"fs": across}).wait_recv()
            return gfin[k].astype(F32)

        @pl.when(inside)
        def _():
            total[...] = gpart[0, y].astype(F32) + fetched(0)

        if levels > 3:
            @pl.when(ends)
            def _():
                total[...] = gsend[z, y].astype(F32) + fetched(0) + fetched(1) + fetched(2)

        sums = []
        for side, refs in ((0, (nfv, nsv)), (1, (nfo, nso))):
            grad = total[:, side * columns:(side + 1) * columns]
            new_first, new_second, direction = adapt(old[2 * side], old[2 * side + 1], grad)
            refs[0][...] = new_first
            refs[1][...] = new_second
            dall[me, :, side * columns:(side + 1) * columns] = direction
            sums.append(jnp.sum(jnp.square(direction.astype(F32))))
        chain["dirs"] = spread(lambda block: dall.at[block], d_send, d_recv)
        row = lax.broadcasted_iota(jnp.int32, sq.shape[1:], 0)
        sq[tp] = jnp.where(row == 0, sums[0], sums[1])
        chain["sq"] = [
            go(remote(sq.at[tp], sq.at[tp], q_send.at[d], q_recv.at[d], {"tp": lax.rem(tp + d, t)}))
            for d in range(1, t)
        ]

    def hook_dirs():
        chain["dirs"] = pass_on(chain["dirs"], lambda block: dall.at[block], d_send, d_recv)
        for copy in chain["sq"]:
            copy.wait_recv()
        fsq[me] = jnp.sum(sq[...], axis=0)
        chain["fsq"] = []
        for d in range(1, n):
            target = lax.rem(me + d, n)
            chain["fsq"].append(go(remote(fsq.at[me], fsq.at[me], s_send.at[d], s_recv.at[d], {"fs": target})))

    def hook_scales():
        for copy in chain["dirs"]:
            copy.wait_recv()
        for side in (0, 1):
            for k in range(n):
                dir32[k * rr:(k + 1) * rr] = dall[k, :, side * columns:(side + 1) * columns].astype(F32)
            dirs[side] = dir32[...].astype(BF16)
        for copy in chain["fsq"]:
            copy.wait_recv()
        chain["whole"].wait_recv()
        totals = jnp.sum(fsq[...], axis=0)
        spread_scales = lax.rsqrt(totals / float(rank * columns * t) + norm_eps)
        for side in (0, 1):
            scales[side] = jnp.broadcast_to(spread_scales[side:side + 1], scales.shape[1:])

    hooks = dict(zip(HOOKS, (
        hook_pass, hook_share, hook_grads, hook_first, hook_second,
        hook_partial, hook_moments, hook_dirs, hook_scales,
    )))
    chain["shared"] = []
    chain["proj"] = spread(part, p_send, p_recv)
    for side in (0, 1):
        weights[side].wait()
        wall[me, base[side]:base[side] + q] = own[side].astype(BF16)
    units = plan() if streamed else []
    end = max(slots, max(HOOKS) + 1, len(line) + LATE)
    for slot in range(end):
        if slot in hooks:
            hooks[slot]()
        advance(slot)
        if slot >= max(HOOKS):
            for _ in range(UNITS):
                if units and units[0][0] <= slot:
                    _, _, work, args = units.pop(0)
                    work(*args)
    for _, _, work, args in units:
        work(*args)
    drained(end, end)

    for k in range(1, levels):
        for i in range(count):
            ensure(0, k, i)
        for i in range(count - early, count):
            ensure(1, k, i)
    for i in range(count - early, count):
        ensure(1, 0, i)
    for j in range(levels):
        for i in range(count - early):
            crossed(j, i)
    if not streamed:
        def whole_block(block, carry):
            for side in (0, 1):
                renew(block, side, 0, q)
            return carry

        lax.fori_loop(0, n, whole_block, 0)
        for side in (0, 1):
            renew_own(side)
    if not (streamed and paired):
        def one_chunk(chunk, carry):
            turn(chunk)
            return carry

        lax.fori_loop(0, n * q // LANES, one_chunk, 0)
    for copy in sends:
        copy.wait_send()
    for d in range(1, levels):
        scatter(d, "wait")
    final(ends, gsend.at[z, 1 - y], 0, across, "wait")
    finals("wait")


def finish(*refs):
    sem, count = refs[-1], len(refs) // 2
    copies = []
    for src, dst in zip(refs[:count], refs[count:]):
        rows = src.shape[0]
        parts = SPLIT if rows % (16 * SPLIT) == 0 else 1
        for p in range(parts):
            place = pl.ds(p * (rows // parts), rows // parts)
            copies.append(pltpu.make_async_copy(src.at[place], dst.at[place], sem.at[len(copies)]))
    for copy in copies:
        copy.start()
    for copy in copies:
        copy.wait()


def per_device(
    n, t,
    inputs, value_cot, retained, output_cot, proj_value, proj_output, w_value, w_output,
    first_value, second_value, first_output, second_output,
):
    tokens, width = inputs.shape
    q, rank = proj_value.shape
    columns = value_cot.shape[1]
    rr = first_value.shape[0]
    levels = n // 2
    pieces = len(cut(2 * q)[0]) - 1
    ways = share(q, t)
    hbm = pl.BlockSpec(memory_space=pltpu.HBM)
    vmem = pl.BlockSpec(memory_space=pltpu.VMEM)
    anywhere = pl.BlockSpec(memory_space=pl.ANY)
    dma = pltpu.SemaphoreType.DMA
    results = pl.pallas_call(
        functools.partial(exchange, n, t),
        out_shape=(
            pltpu.VMEM((n, q, columns), BF16),
            pltpu.VMEM((columns, n * q), BF16),
            pltpu.VMEM((q, columns), F32),
            pltpu.VMEM((q, columns), F32),
            pltpu.VMEM((rr, columns), F32),
            pltpu.VMEM((rr, columns), F32),
            pltpu.VMEM((rr, columns), F32),
            pltpu.VMEM((rr, columns), F32),
        ),
        in_specs=[hbm] * 12,
        out_specs=(vmem,) * 8,
        scratch_shapes=[
            pltpu.VMEM((n, 2 * q, columns), BF16),
            pltpu.VMEM((n, q, columns), BF16),
            pltpu.VMEM((2, q, columns), F32),
            pltpu.VMEM((2, n, q, rank), BF16),
            pltpu.VMEM((tokens, width), BF16),
            pltpu.VMEM((2, tokens, columns), BF16),
            pltpu.VMEM((4, rr, columns), F32),
            pltpu.VMEM((2, tokens, rank), BF16),
            pltpu.VMEM((levels, 2, rr, 2 * columns), BF16),
            pltpu.VMEM((2, levels, 2, rr, 2 * columns), BF16),
            pltpu.VMEM((2, 2, rr, 2 * columns), BF16),
            pltpu.VMEM((3, rr, 2 * columns), BF16),
            pltpu.VMEM((rr, 2 * columns), F32),
            pltpu.VMEM((n, rr, 2 * columns), BF16),
            pltpu.VMEM((rank, columns), F32),
            pltpu.VMEM((2, rank, columns), BF16),
            pltpu.VMEM((t, 8, 128), F32),
            pltpu.VMEM((n, 8, 128), F32),
            pltpu.VMEM((2, 8, 128), F32),
            dma((10,)), dma((n,)), dma((n,)), dma((ways, n)), dma((ways, n)), dma((2,)), dma((2,)),
            dma((levels,)), dma((2, levels)), dma((3,)), dma((3,)), dma((n,)), dma((n,)),
            dma((t,)), dma((t,)), dma((n,)), dma((n,)),
            dma((DEEP,)), dma((DEEP,)), dma((DEPTH,)), dma((2, levels, pieces)),
        ],
        compiler_params=pltpu.CompilerParams(
            collective_id=0, has_side_effects=True, vmem_limit_bytes=51 * 1024 * 1024
        ),
        name="exchange",
    )(
        inputs, output_cot, value_cot, retained, proj_value, proj_output, w_value, w_output.T,
        first_value, second_value, first_output, second_output,
    )
    full = n * q
    values = (results[0].reshape(full, columns),) + tuple(results[1:])
    copy_v, copy_o, step_v, step_o, first_v, second_v, first_o, second_o = pl.pallas_call(
        finish,
        out_shape=tuple(jax.ShapeDtypeStruct(value.shape, value.dtype) for value in values),
        in_specs=[anywhere] * 8,
        out_specs=(anywhere,) * 8,
        scratch_shapes=[dma((8 * SPLIT,))],
        compiler_params=pltpu.CompilerParams(vmem_limit_bytes=12 * 1024 * 1024),
        name="finish",
    )(*values)
    return (step_v, step_o.T, copy_v, copy_o, first_v, second_v, first_o, second_o)


def solution(mesh):
    in_specs = (
        P("fs", None),
        P("fs", "tp"),
        P("fs", "tp"),
        P("fs", None),
        P("fs", None),
        P("fs", None),
        P("fs", "tp"),
        P("tp", "fs"),
        P("fs", "tp"),
        P("fs", "tp"),
        P("fs", "tp"),
        P("fs", "tp"),
    )
    out_specs = (
        P("fs", "tp"),
        P("tp", "fs"),
        P(None, "tp"),
        P("tp", None),
        P("fs", "tp"),
        P("fs", "tp"),
        P("fs", "tp"),
        P("fs", "tp"),
    )
    return jax.shard_map(
        functools.partial(per_device, mesh.shape["fs"], mesh.shape["tp"]),
        mesh=mesh, in_specs=in_specs, out_specs=out_specs, check_vma=False,
    )
```

```python
import functools

import jax
import jax.numpy as jnp
from jax import lax
from jax.experimental import pallas as pl
from jax.experimental.pallas import tpu as pltpu
from jax.sharding import PartitionSpec as P

BF16 = jnp.bfloat16
F32 = jnp.float32

beta_one = 0.8
beta_two = 0.9
moment_eps = 1e-08
norm_eps = 1e-06

PIECES = 12
SHARE = 0.2
DEPTH = 5
HOOKS = (2, 5, 11, 12, 13, 20, 25, 31, 36)
LAG = 3
UNITS = 4
LANES = 128
DEEP = 12
LATE = 1
SPLIT = 2
STREAMED = 8


def adapt(first, second, grad):
    new_first = beta_one * first + (1.0 - beta_one) * grad
    new_second = beta_two * second + (1.0 - beta_two) * grad * grad
    direction = (new_first / (jnp.sqrt(new_second) + moment_eps)).astype(BF16)
    return (new_first, new_second, direction)


def flat(block):
    parts, rows, columns = block.shape
    if rows % 16 == 0:
        return block.reshape(parts * rows, columns)
    return block.astype(F32).reshape(parts * rows, columns).astype(block.dtype)


def cut(rows):
    if rows % (16 * PIECES) == 0:
        ahead = max(32, int(rows * SHARE) // 16 * 16)
        late, size = rows - ahead, rows // PIECES
        return list(range(0, late, size)) + [late, late + ahead // 32 * 16, rows], 2
    edges = list(range(0, rows + 1, 16))
    return edges, max(1, int((len(edges) - 1) * SHARE))


def share(q, t):
    ways = t // 2
    return ways if q % (16 * ways) == 0 else 1


def schedule(levels, count, early):
    line, sent = [], {}
    for s in range(levels - 1):
        for i in range(count):
            sent[s + 1, i] = len(line)
            line.append((0, s, i))
        for i in range(count - early, count):
            line.append((1, s, i))
    over = {}
    slot = 0
    for i in list(range(count - early, count)) + list(range(count - early)):
        over[slot] = (0, i)
        slot += 1
    for j in range(1, levels):
        for i in range(count - early):
            slot = max(slot, sent[j, i] + 3)
            over[slot] = (j, i)
            slot += 1
    return line, over, max(len(line), slot)


def exchange(
    n, t, x_ref, oc_ref, vc_ref, ret_ref, pv_ref, po_ref, wv_ref, wo_ref, fv_ref, sv_ref, fo_ref, so_ref,
    copy_v, copy_o, step_v, step_o, nfv, nsv, nfo, nso,
    wall, flip, own, pall, xin, cot, old, pr, gsend, grecv, gpart, gfin, total, dall, dir32, dirs, sq, fsq, scales,
    load_sem, p_send, p_recv, x_send, x_recv, core_send, core_recv, g_send, g_recv, f_send, f_recv,
    d_send, d_recv, q_send, q_recv, s_send, s_recv, up_send, down_send, over_send, w_recv,
):
    me = lax.axis_index("fs")
    tp = lax.axis_index("tp")
    core = lax.rem(tp, 2)
    partner = tp + 1 - 2 * core
    x = tp // 2
    z, y = me // 2, lax.rem(me, 2)
    levels = n // 2
    across = me + 1 - 2 * y
    q, columns = wv_ref.shape
    rows = 2 * q
    rr, rank = fv_ref.shape[0], pv_ref.shape[1]
    edges, early = cut(rows)
    count = len(edges) - 1
    size = edges[1]
    ways = share(q, t)
    part_rows = q // ways
    streamed = levels <= STREAMED
    paired = levels == 4 and 4 * q % LANES == 0
    base = (q, 0)

    def remote(src, dst, ssem, rsem, device):
        return pltpu.make_async_remote_copy(
            src_ref=src, dst_ref=dst, send_sem=ssem, recv_sem=rsem,
            device_id=device, device_id_type=pl.DeviceIdType.MESH,
        )

    barrier = pltpu.get_barrier_semaphore()
    for d in range(1, n):
        pl.semaphore_signal(
            barrier, inc=1, device_id={"fs": lax.rem(me + d, n)}, device_id_type=pl.DeviceIdType.MESH
        )
    for d in range(1, t):
        pl.semaphore_signal(
            barrier, inc=1, device_id={"tp": lax.rem(tp + d, t)}, device_id_type=pl.DeviceIdType.MESH
        )

    @pl.when(core == 0)
    def _():
        pltpu.make_async_copy(pv_ref, pall.at[0, me], load_sem.at[0]).start()

    @pl.when(core == 1)
    def _():
        pltpu.make_async_copy(po_ref, pall.at[1, me], load_sem.at[0]).start()

    def load(src, dst, k):
        copy = pltpu.make_async_copy(src, dst, load_sem.at[k])
        copy.start()
        return copy

    weights = [load(wv_ref, own.at[0], 1), load(wo_ref, own.at[1], 2)]

    @pl.when(core == 0)
    def _():
        pltpu.make_async_copy(x_ref, xin, load_sem.at[3]).start()

    @pl.when(core == 1)
    def _():
        pltpu.make_async_copy(oc_ref, xin, load_sem.at[3]).start()

    cots = [load(vc_ref, cot.at[0], 4), load(ret_ref, cot.at[1], 5)]
    olds = [load(ref, old.at[k], 6 + k) for k, ref in enumerate((fv_ref, sv_ref, fo_ref, so_ref))]

    for side in (0, 1):
        weights[side].wait()
        wall[me, base[side]:base[side] + q] = own[side].astype(BF16)
    pltpu.make_async_copy(pv_ref, pall.at[core, me], load_sem.at[0]).wait()
    pl.semaphore_wait(barrier, n - 1 + t - 1)

    sends = []

    def go(copy):
        copy.start()
        sends.append(copy)
        return copy

    def spread(place, ssem, rsem):
        mine = place(me)
        first = [go(remote(mine, mine, ssem.at[0], rsem.at[0], {"fs": across}))]
        for d in range(1, levels):
            target = lax.rem(z + d, levels) * 2 + y
            first.append(go(remote(mine, mine, ssem.at[d], rsem.at[d], {"fs": target})))
        return first

    def pass_on(first, place, ssem, rsem):
        second = []
        for d in range(1, levels):
            first[d].wait_recv()
            block = place(lax.rem(z + levels - d, levels) * 2 + y)
            second.append(
                go(remote(block, block, ssem.at[levels + d], rsem.at[levels + d], {"fs": across}))
            )
        return first[:1] + second

    line, over, slots = schedule(levels, count, early)

    def piece(level, side, i):
        column = y if side == 0 else 1 - y
        return wall.at[level * 2 + column, pl.ds(edges[i], edges[i + 1] - edges[i])]

    def along(slot, step):
        side, s, i = line[slot]
        level = z - s if step > 0 else z + s
        place = piece(level, side, i)
        ssem = (up_send if step > 0 else down_send).at[slot % DEEP]
        return remote(place, place, ssem, w_recv.at[side, level, i], {"fs": (z + step) * 2 + y})

    def goes(slot, step):
        s = line[slot][1]
        if step > 0:
            return jnp.logical_and(z >= s, z < levels - 1)
        return jnp.logical_and(z + s < levels, z > 0)

    def nearest(j):
        if j == 0:
            return z
        low = jnp.minimum(z, levels - 1 - z)
        near = z + (j + 1) // 2 * (1 if j % 2 else -1)
        far = jnp.where(z < levels - 1 - z, j, levels - 1 - j)
        return jnp.where(j <= 2 * low, near, far)

    def crossing(slot):
        j, i = over[slot]
        level = nearest(j)
        place = piece(level, 0, i)
        return remote(place, place, over_send.at[slot % DEPTH], w_recv.at[1, level, i], {"fs": across})

    held = set()

    def covering(start, stop):
        return [i for i in range(count) if edges[i] < stop and edges[i + 1] > start]

    def landed(side, level, i):
        place = piece(level, side, i)
        remote(place, place, over_send.at[0], w_recv.at[side, level, i], {"fs": across}).wait_recv()

    def ensure(side, k, i):
        if (side, k, i) in held:
            return
        held.add((side, k, i))
        if k == 0:
            landed(side, z, i)
            return

        @pl.when(z >= k)
        def _():
            landed(side, z - k, i)

        @pl.when(z + k < levels)
        def _():
            landed(side, z + k, i)

    def crossed(j, i):
        if ("over", j, i) not in held:
            held.add(("over", j, i))
            landed(1, nearest(j), i)

    def tight(step):
        return z + step == (levels - 1 if step > 0 else 0)

    done = {"tight": 0, "loose": 0, "over": 0}

    def drained(close, loose):
        for kind, limit in (("tight", close), ("loose", loose)):
            for slot in range(done[kind], min(limit, len(line))):
                for step in (1, -1):
                    paced = tight(step) if kind == "tight" else jnp.logical_not(tight(step))

                    @pl.when(jnp.logical_and(goes(slot, step), paced))
                    def _():
                        along(slot, step).wait_send()
            done[kind] = max(done[kind], limit)
        for slot in range(done["over"], close):
            if slot in over:
                crossing(slot).wait_send()
        done["over"] = max(done["over"], close)

    def advance(slot):
        drained(slot - DEPTH + 1, slot - DEEP + 1)
        if slot < len(line):
            side, s, i = line[slot]
            if side == 1 or s > 0:
                ensure(side, s, i)
            for step in (1, -1):
                @pl.when(jnp.logical_and(goes(slot, step), tight(step)))
                def _():
                    along(slot, step).start()
        if 0 <= slot - LATE < len(line):
            for step in (1, -1):
                @pl.when(jnp.logical_and(goes(slot - LATE, step), jnp.logical_not(tight(step))))
                def _():
                    along(slot - LATE, step).start()
        if slot in over:
            j, i = over[slot]
            for k in range(1, j + 1):
                ensure(0, k, i)
            crossing(slot).start()

    steps = (step_v, step_o)

    def keep(block, side, low, high, value):
        if side == 0:
            copy_v[block, low:high] = value.astype(BF16)
        else:
            flip[block, low:high] = value.astype(BF16)

    def turn(chunk):
        start = pl.multiple_of(chunk * LANES, LANES)
        tile = flip.reshape(n * q, columns)[pl.ds(start, LANES)]
        copy_o[:, pl.ds(start, LANES)] = tile.astype(F32).T.astype(BF16)

    def moved(block, side, low, high):
        part = jnp.dot(pall[side, block, low:high], dirs[side], preferred_element_type=F32)
        return part * scales[side, 0:1, 0:1]

    def renew(block, side, low, high):
        old_part = wall[block, base[side] + low:base[side] + high].astype(F32)
        keep(block, side, low, high, old_part + moved(block, side, low, high))

    def renew_own(side):
        step = moved(me, side, 0, q)
        steps[side][...] = step
        keep(me, side, 0, q, own[side] + step)

    def unit(side, j, half, low, high):
        if side == 0 and j == 0:
            renew_own(half)
            return
        for i in covering(base[half] + low, base[half] + high):
            if side == 1 and (i < count - early or j == 0):
                if i < count - early:
                    crossed(j, i)
                else:
                    ensure(1, 0, i)
            else:
                for k in range(1, j + 1):
                    ensure(side, k, i)
        renew(nearest(j) * 2 + (y if side == 0 else 1 - y), half, low, high)

    def plan():
        at_line = {item: slot for slot, item in enumerate(line)}
        at_over = {item: slot for slot, item in over.items()}
        units, flipped = [], [0] * levels

        def add(ready, work, *args):
            units.append((ready, len(units), work, args))

        for j in range(levels):
            for half in (1, 0):
                for side in (0, 1):
                    fine = 2 * size if j == levels - 1 and q % (2 * size) == 0 else q
                    for low in range(0, q, fine):
                        ready, start = 0, base[half] + low
                        for i in covering(start, start + fine):
                            if side == 1 and (j == 0 or i < count - early):
                                ready = max(ready, at_over[j, i] + LAG)
                            elif j > 0:
                                ready = max(ready, at_line[side, j - 1, i] + LAG)
                        if half == 1:
                            flipped[j] = max(flipped[j], ready)
                        add(ready, unit, side, j, half, low, low + fine)
            if paired and j >= 2:
                group = 4 * q // LANES
                near = z // 2
                low = jnp.where(z < 2, 0, 1)
                split = 2 * q // LANES
                rest = group - split
                if j == 2:
                    for c in range(group):
                        add(max(flipped[:3]), turn, near * group + c)
                    for c in range(split):
                        add(max(flipped[:3]), turn, (1 - near) * group + low * rest + c)
                else:
                    for c in range(rest):
                        add(max(flipped), turn, (1 - near) * group + (1 - low) * split + c)
        return sorted(units, key=lambda item: item[:2])

    chain = {}

    def part(block):
        return pall.at[core, block, pl.ds(x * part_rows, part_rows)]

    def shared(block):
        for d in range(1, ways):
            place = part(block)
            target = lax.rem(x + d, ways) * 2 + core
            chain["shared"].append(
                go(remote(place, place, x_send.at[d, block], x_recv.at[d, block], {"tp": target}))
            )

    def hook_pass():
        first = chain["proj"]
        second = pass_on(first, part, p_send, p_recv)
        for d in range(1, levels):
            shared(lax.rem(z + levels - d, levels) * 2 + y)
        chain["proj"] = second

    def hook_share():
        second = chain["proj"]
        for d, copy in enumerate(second):
            copy.wait_recv()
            shared(lax.rem(z + levels - d, levels) * 2 + 1 - y)

    def hook_grads():
        for copy in chain["shared"]:
            copy.wait_recv()
        chain["whole"] = go(
            remote(pall.at[core], pall.at[core], core_send.at[0], core_recv.at[0], {"tp": partner})
        )
        pltpu.make_async_copy(x_ref, xin, load_sem.at[3]).wait()
        pr[core] = jnp.dot(xin[...], flat(pall[core]), preferred_element_type=F32).astype(BF16)
        chain["swap"] = go(
            remote(pr.at[core], pr.at[core], core_send.at[1], core_recv.at[1], {"tp": partner})
        )

    def project(side):
        grad = lax.dot_general(
            pr[side], cot[side], (((0,), (0,)), ((), ())), preferred_element_type=F32
        )
        for peer in range(n):
            gsend[peer // 2, peer % 2, :, side * columns:(side + 1) * columns] = (
                grad[peer * rr:(peer + 1) * rr].astype(BF16)
            )

    def hook_first():
        for copy in cots:
            copy.wait()
        chain["swap"].wait_recv()
        project(0)

    def hook_second():
        project(1)
        for d in range(1, levels):
            scatter(d, "start")
        final(ends, gsend.at[z, 1 - y], 0, across, "start")

    inside = jnp.logical_and(z > 0, z < levels - 1) if levels > 3 else z >= 0
    ends = jnp.logical_not(inside)

    def scatter(d, act):
        level = lax.rem(z + d, levels)

        def send(kind, owner):
            copy = remote(
                gsend.at[level], grecv.at[kind, z], g_send.at[d], g_recv.at[kind, z], {"fs": owner * 2 + y}
            )
            copy.start() if act == "start" else copy.wait_send()

        if levels < 4:
            send(0, level)
            return
        inner = jnp.logical_and(level > 0, level < levels - 1)
        owner = jnp.where(level == 0, 1, levels - 2)

        @pl.when(inner)
        def _():
            send(0, level)

        @pl.when(jnp.logical_and(jnp.logical_not(inner), z != owner))
        def _():
            send(1, owner)

    def final(when, src, k, peer, act):
        @pl.when(when)
        def _():
            copy = remote(src, gfin.at[k], f_send.at[k], f_recv.at[k], {"fs": peer})
            copy.start() if act == "start" else copy.wait_send()

    def arrived(kind, d):
        level = lax.rem(z + d, levels)
        place = grecv.at[kind, level]
        remote(place, place, g_send.at[d], g_recv.at[kind, level], {"fs": across}).wait_recv()
        return place[...].astype(F32)

    def finals(act):
        final(inside, gpart.at[0, 1 - y], 0, across, act)
        if levels > 3:
            for own_level, end in ((1, 0), (levels - 2, levels - 1)):
                final(z == own_level, gpart.at[1, y], 1, end * 2 + y, act)
                final(z == own_level, gpart.at[1, 1 - y], 2, end * 2 + 1 - y, act)

    def hook_partial():
        @pl.when(inside)
        def _():
            summed = gsend[z].astype(F32)
            for d in range(1, levels):
                summed += arrived(0, d)
            gpart[0] = summed.astype(BF16)

        if levels > 3:
            for own_level, end, sources in (
                (1, 0, range(1, levels - 1)), (levels - 2, levels - 1, range(2, levels))
            ):
                @pl.when(z == own_level)
                def _():
                    summed = gsend[end].astype(F32)
                    for d in sources:
                        summed += arrived(1, d)
                    gpart[1] = summed.astype(BF16)

        finals("start")

    def hook_moments():
        for copy in olds:
            copy.wait()

        def fetched(k):
            remote(gfin.at[k], gfin.at[k], f_send.at[k], f_recv.at[k], {"fs": across}).wait_recv()
            return gfin[k].astype(F32)

        @pl.when(inside)
        def _():
            total[...] = gpart[0, y].astype(F32) + fetched(0)

        if levels > 3:
            @pl.when(ends)
            def _():
                total[...] = gsend[z, y].astype(F32) + fetched(0) + fetched(1) + fetched(2)

        sums = []
        for side, refs in ((0, (nfv, nsv)), (1, (nfo, nso))):
            grad = total[:, side * columns:(side + 1) * columns]
            new_first, new_second, direction = adapt(old[2 * side], old[2 * side + 1], grad)
            refs[0][...] = new_first
            refs[1][...] = new_second
            dall[me, :, side * columns:(side + 1) * columns] = direction
            sums.append(jnp.sum(jnp.square(direction.astype(F32))))
        chain["dirs"] = spread(lambda block: dall.at[block], d_send, d_recv)
        row = lax.broadcasted_iota(jnp.int32, sq.shape[1:], 0)
        sq[tp] = jnp.where(row == 0, sums[0], sums[1])
        chain["sq"] = [
            go(remote(sq.at[tp], sq.at[tp], q_send.at[d], q_recv.at[d], {"tp": lax.rem(tp + d, t)}))
            for d in range(1, t)
        ]

    def hook_dirs():
        chain["dirs"] = pass_on(chain["dirs"], lambda block: dall.at[block], d_send, d_recv)
        for copy in chain["sq"]:
            copy.wait_recv()
        fsq[me] = jnp.sum(sq[...], axis=0)
        chain["fsq"] = []
        for d in range(1, n):
            target = lax.rem(me + d, n)
            chain["fsq"].append(go(remote(fsq.at[me], fsq.at[me], s_send.at[d], s_recv.at[d], {"fs": target})))

    def hook_scales():
        for copy in chain["dirs"]:
            copy.wait_recv()
        for side in (0, 1):
            for k in range(n):
                dir32[k * rr:(k + 1) * rr] = dall[k, :, side * columns:(side + 1) * columns].astype(F32)
            dirs[side] = dir32[...].astype(BF16)
        for copy in chain["fsq"]:
            copy.wait_recv()
        chain["whole"].wait_recv()
        totals = jnp.sum(fsq[...], axis=0)
        spread_scales = lax.rsqrt(totals / float(rank * columns * t) + norm_eps)
        for side in (0, 1):
            scales[side] = jnp.broadcast_to(spread_scales[side:side + 1], scales.shape[1:])

    hooks = dict(zip(HOOKS, (
        hook_pass, hook_share, hook_grads, hook_first, hook_second,
        hook_partial, hook_moments, hook_dirs, hook_scales,
    )))
    chain["shared"] = []
    chain["proj"] = spread(part, p_send, p_recv)
    units = plan() if streamed else []
    end = max(slots, max(HOOKS) + 1, len(line) + LATE)
    for slot in range(end):
        if slot in hooks:
            hooks[slot]()
        advance(slot)
        if slot >= max(HOOKS):
            for _ in range(UNITS):
                if units and units[0][0] <= slot:
                    _, _, work, args = units.pop(0)
                    work(*args)
    for _, _, work, args in units:
        work(*args)
    drained(end, end)

    for k in range(1, levels):
        for i in range(count):
            ensure(0, k, i)
        for i in range(count - early, count):
            ensure(1, k, i)
    for i in range(count - early, count):
        ensure(1, 0, i)
    for j in range(levels):
        for i in range(count - early):
            crossed(j, i)
    if not streamed:
        def whole_block(block, carry):
            for side in (0, 1):
                renew(block, side, 0, q)
            return carry

        lax.fori_loop(0, n, whole_block, 0)
        for side in (0, 1):
            renew_own(side)
    if not (streamed and paired):
        def one_chunk(chunk, carry):
            turn(chunk)
            return carry

        lax.fori_loop(0, n * q // LANES, one_chunk, 0)
    for copy in sends:
        copy.wait_send()
    for d in range(1, levels):
        scatter(d, "wait")
    final(ends, gsend.at[z, 1 - y], 0, across, "wait")
    finals("wait")


def finish(*refs):
    sem, count = refs[-1], len(refs) // 2
    copies = []
    for src, dst in zip(refs[:count], refs[count:]):
        rows = src.shape[0]
        parts = SPLIT if rows % (16 * SPLIT) == 0 else 1
        for p in range(parts):
            place = pl.ds(p * (rows // parts), rows // parts)
            copies.append(pltpu.make_async_copy(src.at[place], dst.at[place], sem.at[len(copies)]))
    for copy in copies:
        copy.start()
    for copy in copies:
        copy.wait()


def per_device(
    n, t,
    inputs, value_cot, retained, output_cot, proj_value, proj_output, w_value, w_output,
    first_value, second_value, first_output, second_output,
):
    tokens, width = inputs.shape
    q, rank = proj_value.shape
    columns = value_cot.shape[1]
    rr = first_value.shape[0]
    levels = n // 2
    pieces = len(cut(2 * q)[0]) - 1
    ways = share(q, t)
    hbm = pl.BlockSpec(memory_space=pltpu.HBM)
    vmem = pl.BlockSpec(memory_space=pltpu.VMEM)
    anywhere = pl.BlockSpec(memory_space=pl.ANY)
    dma = pltpu.SemaphoreType.DMA
    results = pl.pallas_call(
        functools.partial(exchange, n, t),
        out_shape=(
            pltpu.VMEM((n, q, columns), BF16),
            pltpu.VMEM((columns, n * q), BF16),
            pltpu.VMEM((q, columns), F32),
            pltpu.VMEM((q, columns), F32),
            pltpu.VMEM((rr, columns), F32),
            pltpu.VMEM((rr, columns), F32),
            pltpu.VMEM((rr, columns), F32),
            pltpu.VMEM((rr, columns), F32),
        ),
        in_specs=[hbm] * 12,
        out_specs=(vmem,) * 8,
        scratch_shapes=[
            pltpu.VMEM((n, 2 * q, columns), BF16),
            pltpu.VMEM((n, q, columns), BF16),
            pltpu.VMEM((2, q, columns), F32),
            pltpu.VMEM((2, n, q, rank), BF16),
            pltpu.VMEM((tokens, width), BF16),
            pltpu.VMEM((2, tokens, columns), BF16),
            pltpu.VMEM((4, rr, columns), F32),
            pltpu.VMEM((2, tokens, rank), BF16),
            pltpu.VMEM((levels, 2, rr, 2 * columns), BF16),
            pltpu.VMEM((2, levels, 2, rr, 2 * columns), BF16),
            pltpu.VMEM((2, 2, rr, 2 * columns), BF16),
            pltpu.VMEM((3, rr, 2 * columns), BF16),
            pltpu.VMEM((rr, 2 * columns), F32),
            pltpu.VMEM((n, rr, 2 * columns), BF16),
            pltpu.VMEM((rank, columns), F32),
            pltpu.VMEM((2, rank, columns), BF16),
            pltpu.VMEM((t, 8, 128), F32),
            pltpu.VMEM((n, 8, 128), F32),
            pltpu.VMEM((2, 8, 128), F32),
            dma((10,)), dma((n,)), dma((n,)), dma((ways, n)), dma((ways, n)), dma((2,)), dma((2,)),
            dma((levels,)), dma((2, levels)), dma((3,)), dma((3,)), dma((n,)), dma((n,)),
            dma((t,)), dma((t,)), dma((n,)), dma((n,)),
            dma((DEEP,)), dma((DEEP,)), dma((DEPTH,)), dma((2, levels, pieces)),
        ],
        compiler_params=pltpu.CompilerParams(
            collective_id=0, has_side_effects=True, vmem_limit_bytes=51 * 1024 * 1024
        ),
        name="exchange",
    )(
        inputs, output_cot, value_cot, retained, proj_value, proj_output, w_value, w_output.T,
        first_value, second_value, first_output, second_output,
    )
    full = n * q
    values = (results[0].reshape(full, columns),) + tuple(results[1:])
    copy_v, copy_o, step_v, step_o, first_v, second_v, first_o, second_o = pl.pallas_call(
        finish,
        out_shape=tuple(jax.ShapeDtypeStruct(value.shape, value.dtype) for value in values),
        in_specs=[anywhere] * 8,
        out_specs=(anywhere,) * 8,
        scratch_shapes=[dma((8 * SPLIT,))],
        compiler_params=pltpu.CompilerParams(vmem_limit_bytes=12 * 1024 * 1024),
        name="finish",
    )(*values)
    return (step_v, step_o.T, copy_v, copy_o, first_v, second_v, first_o, second_o)


def solution(mesh):
    in_specs = (
        P("fs", None),
        P("fs", "tp"),
        P("fs", "tp"),
        P("fs", None),
        P("fs", None),
        P("fs", None),
        P("fs", "tp"),
        P("tp", "fs"),
        P("fs", "tp"),
        P("fs", "tp"),
        P("fs", "tp"),
        P("fs", "tp"),
    )
    out_specs = (
        P("fs", "tp"),
        P("tp", "fs"),
        P(None, "tp"),
        P("tp", None),
        P("fs", "tp"),
        P("fs", "tp"),
        P("fs", "tp"),
        P("fs", "tp"),
    )
    return jax.shard_map(
        functools.partial(per_device, mesh.shape["fs"], mesh.shape["tp"]),
        mesh=mesh, in_specs=in_specs, out_specs=out_specs, check_vma=False,
    )
```
